1024 devices in a mesh: ep: 32 (over z, core), tp: 32 (over y, x).
Axes of the slice: x: 4, y: 8, z: 16, core: 2. Of those that a mesh axis runs over, the one named last changes fastest.
Arguments:
- tokens: bfloat16 [4096, 2048], P('ep'), may hold values from -6 to 6
- cotangent: bfloat16 [4096, 2048], P('ep'), may hold values from -6 to 6
- routes: int32 [4096, 2], P('ep'), may hold values from 0 to 31, all different within a row; in each aligned block of 128 rows (0 to 127, 128 to 255, ...) at most 16 rows name the same one
- route_weight: float32 [4096, 2], P('ep'), may hold values from 0.1 to 1
- w_gate: bfloat16 [32, 2048, 1024], P('ep', None, 'tp'), may hold values from -0.25 to 0.25
- w_up: bfloat16 [32, 2048, 1024], P('ep', None, 'tp'), may hold values from -0.25 to 0.25
- w_down: bfloat16 [32, 1024, 2048], P('ep', 'tp'), may hold values from -0.1875 to 0.1875
Outputs:
- grad_tokens: bfloat16 [4096, 2048], P('ep', 'tp')
- grad_route_weight: float32 [4096, 2], P('ep')
- grad_gate: float32 [32, 2048, 1024], P('ep', None, 'tp')
- grad_up: float32 [32, 2048, 1024], P('ep', None, 'tp')
- grad_down: float32 [32, 1024, 2048], P('ep', 'tp')
The draws below stay inside these ranges and needn't reach their ends.
Inputs may be any that keep to these rules, and one draw needn't show every extreme that they name: `routes`: each row names 2 different experts. In each aligned block of 128 rows (the rows of one index of ep) no expert is named by more than 16 rows, and in every draw some expert is named by exactly 16 rows of some block.
All inputs are finite; a program needn't handle non-finite values.
Results may differ from the reference program's by a relative error of at most 0.023.
Values may be sent and summed in bfloat16 or wider, within the bound.
A program may use at most 32 MiB of HBM per device.

```python
import math
import jax
import jax.numpy as jnp
import numpy as np
from jax import lax

D = 2048
FF = 1024
TOP_K = 2
TOK_DEV = 128
EXPERTS = 32
TOKENS = 4096
CAP = 16
N_EP = 32
N_TP = 32


def strengthened(result, rng, source, target, blocks, factor):
    def block_of(axis_at):
        return (jnp.arange(result.shape[axis_at]) // (result.shape[axis_at] // blocks)).reshape((-1,) + (1,) * (result.ndim - 1 - axis_at))

    near = jax.random.permutation(rng, blocks)[block_of(target)]
    second = (block_of(target) + blocks // 2) % blocks
    return jnp.where((block_of(source) == near) | (block_of(source) == second), factor * result, result)


def levels(rng, shape, cuts, least, top_value):
    def one(dim, shards_of):
        heights = jax.random.uniform(jax.random.fold_in(jax.random.fold_in(rng, 6), dim), (shards_of,), jnp.float32, least / len(cuts), top_value / len(cuts))
        return jnp.repeat(jnp.exp(heights), shape[dim] // shards_of).reshape((-1,) + (1,) * (len(shape) - dim - 1))

    gain = one(*cuts[0])
    for cut in cuts[1:]:
        gain = gain * one(*cut)
    return gain


def routed_block(own_key, own, number, rows, amount, top, bound, slope):
    ranking = jax.random.permutation(own_key, amount)
    packed, common = shares(amount, rows * top, bound, slope, True), shares(amount, rows * top, bound, slope, False)
    places = jnp.arange(amount)

    def named(lengths, rotation):
        used = int((lengths > 0).sum())
        fixed = max(1, used // 4)
        moved = fixed + (places - fixed + rotation * (used - fixed)) % max(1, amount - fixed)
        return jnp.zeros((amount,), jnp.int32).at[ranking[jnp.where(places < fixed, places, moved)]].set(jnp.asarray(lengths, jnp.int32))

    lengths = jnp.where(number % 4 == 0, named(packed, number // 4), named(common, number - number // 4 - 1))
    mixed = jax.random.permutation(jax.random.fold_in(own, 3), amount)
    giver, receiver = mixed[0:amount // 2 * 2:2], mixed[1:amount // 2 * 2:2]
    slack = jnp.minimum(lengths[giver] - 1, bound - lengths[receiver]) // 2
    slack = jnp.where((giver == ranking[0]) | (receiver == ranking[0]) | (lengths[receiver] == 0), 0, jnp.maximum(slack, 0))
    moved = jax.random.randint(jax.random.fold_in(own, 4), (amount // 2,), 0, 1 << 20) % (slack + 1)
    lengths = lengths.at[giver].add(-moved).at[receiver].add(moved)
    members = jnp.searchsorted(jnp.cumsum(lengths), jnp.arange(rows * top), side="right").astype(jnp.int32)
    grid = members.reshape(top, rows).T
    grid = grid[jax.random.permutation(jax.random.fold_in(own, 1), rows)]
    rotation = jax.random.randint(jax.random.fold_in(own, 2), (rows, 1), 0, top)
    return jnp.take_along_axis(grid, (jnp.arange(top)[None, :] + rotation) % top, axis=1)


def shares(number_of, total, bound, lean, full):
    portions = [(1 << 20) // math.isqrt(grade ** lean) + 1 for grade in range(1, number_of + 1)]
    largest = bound if full else min(bound, max(-(-total // number_of), total * portions[0] // sum(portions)))
    least = 1 if total - largest >= number_of - 1 else 0
    holding, surplus = [largest] + [least] * (number_of - 1), total - largest - least * (number_of - 1)
    while surplus > 0:
        free = [i for i in range(1, number_of) if holding[i] < largest] or [i for i in range(1, number_of) if holding[i] < bound]
        pool, budget = sum([portions[i] for i in free]), surplus
        for i in free:
            extra = min(bound - holding[i], max(1, budget * portions[i] // pool), surplus)
            holding[i] = holding[i] + extra
            surplus = surplus - extra
    return np.array(holding)


def scatter_about(stream_key, shape, scale, reach, cuts=(), kind=jnp.bfloat16):
    array = jax.random.normal(stream_key, shape, jnp.float32) * scale
    if len(cuts) > 0:
        array = levels(stream_key, shape, cuts, -0.22, 0.18) * array
    return jnp.clip(array, min=-reach, max=reach).astype(kind)


def gaussian_with(stream_key, shape, spread, reach, shards, heavy, held_as=jnp.bfloat16):
    entries = spread * jax.random.normal(stream_key, shape, jnp.float32)
    if shards:
        entries = entries * levels(stream_key, shape, shards, -0.22, 0.18)
    return jnp.clip(strengthened(entries, jax.random.fold_in(stream_key, 3), *heavy), -reach, reach).astype(held_as)


def setup_inputs(seed: int = 0) -> dict:
    key_list = jax.random.split(jax.random.key(seed), 8)
    tokens = scatter_about(key_list[0], (TOKENS, D), 1.0, 6.0, ((0, 32),))
    cotangent = scatter_about(key_list[1], (TOKENS, D), 1.0, 6.0, ((0, 32),))
    routes_keys = jax.random.split(jax.random.fold_in(key_list[2], 1), TOKENS // TOK_DEV)
    routes_turns = jax.random.permutation(jax.random.fold_in(key_list[2], 3), TOKENS // TOK_DEV)
    routes = jax.vmap(lambda own, number: routed_block(jax.random.fold_in(key_list[2], 2), own, number, TOK_DEV, EXPERTS, TOP_K, CAP, 2))(routes_keys, routes_turns).reshape((TOKENS, TOP_K))
    route_weight = jnp.clip(0.1 + 0.9 * jax.random.uniform(key_list[3], (TOKENS, TOP_K), jnp.float32) ** levels(key_list[3], (TOKENS, TOP_K), ((0, 32),), -0.2, 0.2), 0.1, 1.0)
    w_gate = gaussian_with(key_list[4], (EXPERTS, D, FF), D ** -0.5, 0.25, ((0, 32), (2, 32)), (2, 1, 32, 2.75))
    w_up = gaussian_with(key_list[5], (EXPERTS, D, FF), D ** -0.5, 0.25, ((0, 32), (2, 32)), (2, 1, 32, 2.75))
    w_down = scatter_about(key_list[6], (EXPERTS, FF, D), FF ** -0.5, 0.1875, ((0, 32), (1, 32)))
    return {"tokens": tokens, "cotangent": cotangent, "routes": routes, "route_weight": route_weight, "w_gate": w_gate, "w_up": w_up, "w_down": w_down}


def slot_index(block_routes, experts, capacity):
    flat_ids = block_routes.reshape(-1)
    onehot = (flat_ids[:, None] == jnp.arange(experts, dtype=jnp.int32)[None, :]).astype(jnp.int32)
    earlier = jnp.cumsum(onehot, axis=0) - onehot
    return flat_ids * capacity + jnp.sum(earlier * onehot, axis=1)


def expert_grads(inputs):
    rows_x, rows_dy, rows_w, gate_w, up_w, down_w = inputs
    f32 = jnp.float32
    n_rows, model_width = rows_x.shape
    gate_pre = jnp.dot(rows_x, gate_w, preferred_element_type=f32)
    up_pre = jnp.dot(rows_x, up_w, preferred_element_type=f32)
    gate_sig = jax.nn.sigmoid(gate_pre)
    act_full = gate_pre * gate_sig * up_pre
    act = act_full.astype(jnp.bfloat16)
    back_hidden = jnp.dot(rows_dy, down_w.T, preferred_element_type=f32)
    weighted_cot = (rows_w[:, None] * rows_dy.astype(f32)).astype(jnp.bfloat16)
    d_hidden = rows_w[:, None] * back_hidden
    d_gate = (d_hidden * up_pre * gate_sig * (1.0 + gate_pre * (1.0 - gate_sig))).astype(jnp.bfloat16)
    d_up = (d_hidden * gate_pre * gate_sig).astype(jnp.bfloat16)
    gate_grad = jnp.sum(act_full * back_hidden, axis=1)
    pieces = jnp.einsum('rjf,djf->jrd', d_gate.astype(f32).reshape(n_rows, N_TP, -1),
                        gate_w.astype(f32).reshape(model_width, N_TP, -1), precision=lax.Precision.HIGHEST)
    pieces = pieces + jnp.einsum('rjf,djf->jrd', d_up.astype(f32).reshape(n_rows, N_TP, -1),
                                 up_w.astype(f32).reshape(model_width, N_TP, -1), precision=lax.Precision.HIGHEST)
    rounded = lax.optimization_barrier(pieces.astype(jnp.bfloat16))
    route_grad = jnp.sum(rounded.astype(f32), axis=0).astype(jnp.bfloat16)
    grad_gate_e = jnp.dot(rows_x.T, d_gate, preferred_element_type=f32)
    grad_up_e = jnp.dot(rows_x.T, d_up, preferred_element_type=f32)
    grad_down_e = jnp.dot(act.T, weighted_cot, preferred_element_type=f32)
    return route_grad, gate_grad, grad_gate_e, grad_up_e, grad_down_e


def reference(tokens, cotangent, routes, route_weight, w_gate, w_up, w_down):
    f32 = jnp.float32
    blocks = routes.reshape(N_EP, TOK_DEV, TOP_K)
    slot_ids = jax.vmap(lambda block: slot_index(block, EXPERTS, CAP))(blocks)
    expert_ids = blocks.reshape(N_EP, TOK_DEV * TOP_K)
    positions = slot_ids - expert_ids * CAP
    sources = jnp.arange(N_EP, dtype=jnp.int32)[:, None]
    rows_x = jnp.repeat(tokens.reshape(N_EP, TOK_DEV, D), TOP_K, axis=1)
    rows_dy = jnp.repeat(cotangent.reshape(N_EP, TOK_DEV, D), TOP_K, axis=1)
    rows_w = route_weight.reshape(N_EP, TOK_DEV * TOP_K)
    buf_x = jnp.zeros((EXPERTS, N_EP, CAP, D), jnp.bfloat16).at[expert_ids, sources, positions].set(rows_x)
    buf_dy = jnp.zeros((EXPERTS, N_EP, CAP, D), jnp.bfloat16).at[expert_ids, sources, positions].set(rows_dy)
    buf_w = jnp.zeros((EXPERTS, N_EP, CAP), f32).at[expert_ids, sources, positions].set(rows_w)
    recv_rows = N_EP * CAP
    outs = lax.map(expert_grads, (buf_x.reshape(EXPERTS, recv_rows, D), buf_dy.reshape(EXPERTS, recv_rows, D),
                                  buf_w.reshape(EXPERTS, recv_rows), w_gate, w_up, w_down))
    route_grad, gate_grad, grad_gate, grad_up, grad_down = outs
    back_index = sources * CAP + positions
    picked = route_grad[expert_ids, back_index].astype(f32).reshape(TOKENS, TOP_K, D)
    grad_tokens = jnp.sum(picked, axis=1).astype(jnp.bfloat16)
    grad_route_weight = gate_grad[expert_ids, back_index].reshape(TOKENS, TOP_K)
    return grad_tokens, grad_route_weight, grad_gate, grad_up, grad_down
```

```python
import functools

import jax
import jax.numpy as jnp
from jax import lax
from jax.experimental import pallas as pl
from jax.experimental.pallas import tpu as pltpu
from jax.sharding import PartitionSpec as P

MESH = pl.DeviceIdType.MESH
F32 = jnp.float32
BF16 = jnp.bfloat16
LANES = 128
FEAT = 64
HID = 32
CHUNKS = 4


def dot(a, b, ca, cb):
    return lax.dot_general(a, b, (((ca,), (cb,)), ((), ())), preferred_element_type=F32)


def kernel(
    nz, ny, nx, cap,
    tokens, cotangent, routes, weights, gate_w, up_w, down_w,
    out_tok, out_rw, out_gate, out_up, out_down,
    tok_in, cot_in, gate_in, up_in, down_in,
    onehot0, onehot1, send, rows, w_send, w_all, w_left, w_right,
    part_send, part_got, hidden, piece, piece_got, rw_row, rw_got,
    back, back_got, grad_send, grad_got,
    in_sem, z_send, z_recv, w_ssem, w_rsem, ag_ssem, ag_rsem,
    px_ssem, px_rsem, hx_ssem, hx_rsem, ry_ssem, ry_rsem, rw_ssem, rw_rsem,
    b_ssem, b_rsem, g_ssem, g_rsem,
):
    nep = 2 * nz
    count = nep * cap
    half = count // 2
    tok_dev = tokens.shape[0]
    ep = lax.axis_index("ep")
    tp = lax.axis_index("tp")
    z, core = ep // 2, ep % 2
    y, x = tp // nx, tp % nx

    def remote(src, dst, ssem, rsem, to_ep, to_tp):
        return pltpu.make_async_remote_copy(
            src_ref=src, dst_ref=dst, send_sem=ssem, recv_sem=rsem,
            device_id=(to_ep, to_tp), device_id_type=MESH,
        )

    def arrived(ref, sem):
        pltpu.make_async_copy(ref, ref, sem).wait()

    def ep_peer(i, c):
        k = (i + 1) // 2
        dz = nz // 2 + k - 2 * k * (i % 2)
        return ((z + dz) % nz) * 2 + (core + c) % 2

    def x_peer(d):
        return y * nx + (x + d) % nx

    def y_peer(d):
        return ((y + d) % ny) * nx + x

    def col(i):
        return pl.ds(pl.multiple_of(i * LANES, LANES), LANES)

    def slot(e):
        return pl.ds(pl.multiple_of(e * cap, cap), cap)

    barrier = pltpu.get_barrier_semaphore()

    def greet(to_ep, to_tp):
        pl.semaphore_signal(barrier, inc=1, device_id=(to_ep, to_tp), device_id_type=MESH)

    def greet_ep(i, carry):
        greet(ep_peer(i, 0), tp)
        greet(ep_peer(i, 1), tp)
        return carry

    lax.fori_loop(0, nz - 1, greet_ep, 0)
    greet(ep_peer(nz - 1, 1), tp)
    for d in range(1, nx):
        greet(ep, x_peer(d))
    for d in range(1, ny):
        greet(ep, y_peer(d))

    pair = col(tp // 2)
    loads = [
        pltpu.make_async_copy(tokens.at[:, pair], tok_in, in_sem.at[0]),
        pltpu.make_async_copy(cotangent.at[:, pair], cot_in, in_sem.at[1]),
        pltpu.make_async_copy(gate_w, gate_in, in_sem.at[2]),
        pltpu.make_async_copy(up_w, up_in, in_sem.at[3]),
        pltpu.make_async_copy(down_w, down_in, in_sem.at[4]),
    ]
    for load in loads:
        load.start()

    ids = lax.broadcasted_iota(jnp.int32, (nep, tok_dev), 0)
    first = (routes[0:1, :] == ids).astype(F32)
    second = (routes[1:2, :] == ids).astype(F32)
    named = first + second
    below = (
        lax.broadcasted_iota(jnp.int32, (tok_dev, tok_dev), 0)
        < lax.broadcasted_iota(jnp.int32, (tok_dev, tok_dev), 1)
    ).astype(F32).astype(BF16)
    place = dot(named.astype(BF16), below, 1, 0)
    at_slot = lax.broadcasted_iota(jnp.int32, (nep, cap, tok_dev), 1).astype(F32)

    def spread(value):
        return jnp.broadcast_to(value[:, None, :], (nep, cap, tok_dev))

    hit = (spread(place) == at_slot).astype(F32)
    hot0 = (hit * spread(first)).reshape(count, tok_dev)
    hot1 = (hit * spread(second)).reshape(count, tok_dev)
    onehot0[...] = hot0.astype(BF16)
    onehot1[...] = hot1.astype(BF16)
    row_w = jnp.sum(hot0 * weights[0:1, :] + hot1 * weights[1:2, :], axis=1, keepdims=True)

    loads[0].wait()
    loads[1].wait()
    lane = lax.broadcasted_iota(jnp.int32, (tok_dev, LANES), 1)
    odd = tp % 2
    tok = tok_in[...].astype(F32)
    cot = cot_in[...].astype(F32)
    tok = jnp.where(odd == 1, pltpu.roll(tok, FEAT, 1), tok)
    cot = jnp.where(odd == 1, cot, pltpu.roll(cot, FEAT, 1))
    both = jnp.where(lane < FEAT, tok, cot).astype(BF16)
    sent = dot((hot0 + hot1).astype(BF16), both, 1, 0)
    row_lane = lax.broadcasted_iota(jnp.int32, (count, LANES), 1)
    send[...] = (sent * jnp.where(row_lane < FEAT, 1.0, row_w)).astype(BF16)

    pl.semaphore_wait(barrier, (nep - 1) + (nx - 1) + (ny - 1))

    group = nep // CHUNKS
    my_group = ep // group

    def dispatch(i, c):
        to = ep_peer(i, c)
        remote(
            send.at[slot(to), :], rows.at[slot(ep), col(y)], z_send, z_recv.at[my_group], to, tp
        ).start()

    def dispatch_both(i, carry):
        dispatch(i, 0)
        dispatch(i, 1)
        return carry

    lax.fori_loop(0, nz - 1, dispatch_both, 0)
    dispatch(nz - 1, 1)
    rows[slot(ep), col(y)] = send[slot(ep), :]

    for load in loads[2:]:
        load.wait()
    w_lane = lax.broadcasted_iota(jnp.int32, (HID, LANES), 1)
    zero = jnp.zeros((HID, LANES), F32)
    for t in range(nx * ny):
        tile = slice(t // 2 * LANES, (t // 2 + 1) * LANES)
        to_x, to_tile = t % nx, slice(t // nx * LANES, (t // nx + 1) * LANES)
        for k, ref in enumerate((gate_in, up_in, down_in)):
            value = ref[:, tile].astype(F32)
            if (t % 2 == 0) == (k == 2):
                value = pltpu.roll(value, FEAT, 1)
            keep = (w_lane >= FEAT) if k == 2 else (w_lane < FEAT)
            w_send[to_x, k * HID : (k + 1) * HID, to_tile] = jnp.where(keep, value, zero).astype(BF16)
    w_rows = 3 * HID

    def w_place(i):
        return pl.ds(pl.multiple_of(i * LANES, LANES), w_rows)

    w_copies = []
    for d in range(1, nx):
        to = (x + d) % nx
        copy = remote(
            w_send.at[to], w_all.at[w_place(x), :], w_ssem.at[d], w_rsem.at[d], ep, x_peer(d)
        )
        copy.start()
        w_copies.append(copy)
    w_all[w_place(x), :] = w_send[x]
    for i in range(nx):
        w_all[i * LANES + w_rows : (i + 1) * LANES, :] = jnp.zeros((LANES - w_rows, ny * LANES), BF16)

    steps = ny // 2
    per = count // CHUNKS
    order = [0, 1, 3, 2]

    def chunk_of(i):
        return (my_group + order[i]) % CHUNKS

    def ring(way, step, i, owner):
        place_ = rows.at[pl.ds(pl.multiple_of(chunk_of(i) * per, per), per), col(owner)]
        to = y_peer(1) if way == 0 else y_peer(ny - 1)
        return remote(
            place_, place_, ag_ssem.at[way, step - 1, i], ag_rsem.at[way, step - 1, i], ep, to
        )

    def owner_of(way, back_):
        return (y + ny - back_) % ny if way == 0 else (y + back_) % ny

    def travels(way, step, i):
        return step < steps or (i < CHUNKS // 2) == (way == 0)

    ring_copies = []
    for wave in range(1, steps + CHUNKS):
        for step in range(steps, 0, -1):
            i = wave - step
            if not 0 <= i < CHUNKS:
                continue
            if step == 1:
                chunk = chunk_of(i)
                place_ = rows.at[pl.ds(pl.multiple_of(chunk * per, per), per), col(y)]
                short = rows.at[pl.ds(0, per - cap), col(y)]
                if order[i] == 0:
                    arrived(short, z_recv.at[chunk])
                else:
                    arrived(place_, z_recv.at[chunk])
            for way in (0, 1):
                if step > 1:
                    ring(way, step - 1, i, owner_of(way, step - 1)).wait_recv()
                if travels(way, step, i):
                    copy = ring(way, step, i, owner_of(way, step - 1))
                    copy.start()
                    ring_copies.append(copy)
    for way in (0, 1):
        for i in range(CHUNKS):
            if travels(way, steps, i):
                ring(way, steps, i, owner_of(way, steps)).wait_recv()

    for d in range(1, nx):
        arrived(w_all.at[w_place((x + nx - d) % nx), :], w_rsem.at[d])
    part = dot(rows[...], w_all[...], 1, 1)
    part_send[...] = part.astype(BF16)
    part_copies = []
    for d in range(1, nx):
        copy = remote(
            part_send.at[:, col((x + d) % nx)], part_got.at[d], px_ssem.at[d], px_rsem.at[d],
            ep, x_peer(d),
        )
        copy.start()
        part_copies.append(copy)
    for i in range(nx):
        top = slice(i * LANES, i * LANES + 2 * HID)
        rest = slice(i * LANES + 2 * HID, (i + 1) * LANES)
        w_left[top, :] = w_all[top, :]
        w_left[rest, :] = jnp.zeros((LANES - 2 * HID, ny * LANES), BF16)
        w_right[rest, :] = jnp.zeros((LANES - 2 * HID, ny * LANES), BF16)
        for j in range(ny):
            tile = slice(j * LANES, (j + 1) * LANES)
            w_right[top, tile] = pltpu.roll(w_all[top, tile].astype(F32), FEAT, 1).astype(BF16)
    pre = part_send[:, col(x)].astype(F32)
    for d in range(1, nx):
        arrived(part_got.at[d], px_rsem.at[d])
        pre = pre + part_got[d].astype(F32)
    up = pltpu.roll(pre, LANES - HID, 1)
    d_hidden = pltpu.roll(pre, LANES - 2 * HID, 1)
    sig = jax.nn.sigmoid(pre)
    act = pre * sig * up
    d_gate = d_hidden * up * sig * (1.0 + pre * (1.0 - sig))
    d_up = d_hidden * pre * sig
    rw = jnp.sum(jnp.where(row_lane < HID, act * d_hidden, 0.0), axis=1, keepdims=True)
    packed = jnp.where(
        row_lane < HID,
        d_gate,
        jnp.where(
            row_lane < 2 * HID,
            pltpu.roll(d_up, HID, 1),
            jnp.where(
                row_lane < 3 * HID,
                pltpu.roll(act, 2 * HID, 1),
                jnp.where(row_lane == 3 * HID, rw, 0.0),
            ),
        ),
    )
    hidden[:, col(x)] = packed.astype(BF16)
    hidden_copies = []
    for d in range(1, nx):
        copy = remote(
            hidden.at[:, col(x)], hidden.at[:, col(x)], hx_ssem.at[d], hx_rsem.at[d], ep, x_peer(d)
        )
        copy.start()
        hidden_copies.append(copy)
    for d in range(1, nx):
        arrived(hidden.at[:, col((x + nx - d) % nx)], hx_rsem.at[d])

    pieces = dot(hidden[0:half, :], w_left[...], 1, 0) + dot(hidden[half:count, :], w_right[...], 1, 0)
    piece[...] = pieces.astype(BF16)
    pick = (lax.broadcasted_iota(jnp.int32, (16, nx * LANES), 1) % LANES == 3 * HID).astype(F32).astype(BF16)
    rw_row[...] = dot(pick, hidden[...], 1, 1)[0:1, :]
    y_order = []
    for k in range(ny - 1):
        y_order.append(ny // 2 + (k + 1) // 2 * (1 if k % 2 == 0 else -1))
    piece_copies = []
    for d in y_order:
        copy = remote(
            piece.at[:, col((y + d) % ny)], piece_got.at[d], ry_ssem.at[d], ry_rsem.at[d],
            ep, y_peer(d),
        )
        copy.start()
        piece_copies.append(copy)
        copy = remote(rw_row, rw_got.at[d], rw_ssem.at[d], rw_rsem.at[d], ep, y_peer(d))
        copy.start()
        piece_copies.append(copy)

    grads = dot(hidden[...], rows[...], 0, 0)
    g_lane = lax.broadcasted_iota(jnp.int32, (HID, ny * LANES), 1) % LANES
    for i in range(nx):
        at = i * LANES
        gate_down = jnp.where(g_lane < FEAT, grads[at : at + HID, :], grads[at + 2 * HID : at + 3 * HID, :])
        grad_send[i, 0:HID, :] = gate_down.astype(BF16)
        grad_send[i, HID : 2 * HID, :] = grads[at + HID : at + 2 * HID, :].astype(BF16)
    grad_copies = []
    for d in range(1, nx):
        copy = remote(
            grad_send.at[(x + d) % nx], grad_got.at[x], g_ssem.at[d], g_rsem.at[d], ep, x_peer(d)
        )
        copy.start()
        grad_copies.append(copy)
    grad_got[x] = grad_send[x]

    total = piece[:, col(y)].astype(F32)
    total_rw = rw_row[...]
    for d in y_order[::-1]:
        arrived(piece_got.at[d], ry_rsem.at[d])
        arrived(rw_got.at[d], rw_rsem.at[d])
        total = total + piece_got[d].astype(F32)
        total_rw = total_rw + rw_got[d]
    spread_rw = jnp.broadcast_to(total_rw, (LANES, count)).T
    total = jnp.concatenate([total, pltpu.roll(total, FEAT, 1)], axis=0)
    back[...] = jnp.where(row_lane < FEAT, total, spread_rw).astype(BF16)

    def send_back(i, c):
        to = ep_peer(i, c)
        remote(back.at[slot(to), :], back_got.at[slot(ep), :], b_ssem, b_rsem, to, tp).start()

    def back_both(i, carry):
        send_back(i, 0)
        send_back(i, 1)
        return carry

    lax.fori_loop(0, nz - 1, back_both, 0)
    send_back(nz - 1, 1)
    back_got[slot(ep), :] = back[slot(ep), :]

    for d in range(1, nx):
        arrived(grad_got.at[(x + nx - d) % nx], g_rsem.at[d])
    for t in range(0, nx * ny, 2):
        tile = slice(t // 2 * LANES, (t // 2 + 1) * LANES)
        src = slice(t // nx * LANES, (t // nx + 1) * LANES)
        a, b = t % nx, t % nx + 1
        top_a = grad_got[a, 0:HID, src].astype(F32)
        top_b = grad_got[b, 0:HID, src].astype(F32)
        up_a = grad_got[a, HID : 2 * HID, src].astype(F32)
        up_b = grad_got[b, HID : 2 * HID, src].astype(F32)
        out_gate[:, tile] = jnp.where(w_lane < FEAT, top_a, pltpu.roll(top_b, FEAT, 1))
        out_up[:, tile] = jnp.where(w_lane < FEAT, up_a, pltpu.roll(up_b, FEAT, 1))
        out_down[:, tile] = jnp.where(w_lane < FEAT, pltpu.roll(top_a, FEAT, 1), top_b)

    others = pl.ds(0, (nep - 1) * cap)
    arrived(back_got.at[others, :], b_rsem)
    got = back_got[...]
    by_first = dot(got, onehot0[...], 0, 0)
    by_second = dot(got, onehot1[...], 0, 0)
    out_tok[...] = (by_first[0:FEAT, :] + by_second[0:FEAT, :]).astype(BF16)
    out_rw[0:1, :] = by_first[FEAT : FEAT + 1, :] / weights[0:1, :]
    out_rw[1:2, :] = by_second[FEAT : FEAT + 1, :] / weights[1:2, :]

    arrived(send.at[others, :], z_send)
    arrived(back.at[others, :], b_ssem)
    for copy in w_copies + ring_copies + part_copies + hidden_copies + piece_copies + grad_copies:
        copy.wait_send()


def on_device(nz, ny, nx, tokens, cotangent, routes, route_weight, w_gate, w_up, w_down):
    tok_dev, model = tokens.shape
    hid = w_down.shape[1]
    nep = 2 * nz
    cap = 2 * tok_dev * routes.shape[1] // nep
    count = nep * cap
    half = count // 2
    wide_x, wide_y = nx * LANES, ny * LANES
    steps = ny // 2
    any_ = pl.BlockSpec(memory_space=pl.ANY)
    vmem = pl.BlockSpec(memory_space=pltpu.VMEM)
    dma = pltpu.SemaphoreType.DMA
    outs = pl.pallas_call(
        functools.partial(kernel, nz, ny, nx, cap),
        out_shape=(
            jax.ShapeDtypeStruct((FEAT, tok_dev), BF16),
            jax.ShapeDtypeStruct((2, tok_dev), F32),
            jax.ShapeDtypeStruct((hid, model), F32),
            jax.ShapeDtypeStruct((hid, model), F32),
            jax.ShapeDtypeStruct((hid, model), F32),
        ),
        in_specs=[any_, any_, vmem, vmem, any_, any_, any_],
        out_specs=[vmem] * 5,
        scratch_shapes=[
            pltpu.VMEM((tok_dev, LANES), BF16),
            pltpu.VMEM((tok_dev, LANES), BF16),
            pltpu.VMEM((hid, model), BF16),
            pltpu.VMEM((hid, model), BF16),
            pltpu.VMEM((hid, model), BF16),
            pltpu.VMEM((count, tok_dev), BF16),
            pltpu.VMEM((count, tok_dev), BF16),
            pltpu.VMEM((count, LANES), BF16),
            pltpu.VMEM((count, wide_y), BF16),
            pltpu.VMEM((nx, 3 * HID, wide_y), BF16),
            pltpu.VMEM((wide_x, wide_y), BF16),
            pltpu.VMEM((wide_x, wide_y), BF16),
            pltpu.VMEM((wide_x, wide_y), BF16),
            pltpu.VMEM((count, wide_x), BF16),
            pltpu.VMEM((nx, count, LANES), BF16),
            pltpu.VMEM((count, wide_x), BF16),
            pltpu.VMEM((half, wide_y), BF16),
            pltpu.VMEM((ny, half, LANES), BF16),
            pltpu.VMEM((1, count), F32),
            pltpu.VMEM((ny, 1, count), F32),
            pltpu.VMEM((count, LANES), BF16),
            pltpu.VMEM((count, LANES), BF16),
            pltpu.VMEM((nx, 2 * HID, wide_y), BF16),
            pltpu.VMEM((nx, 2 * HID, wide_y), BF16),
            dma((5,)),
            dma,
            dma((CHUNKS,)),
            dma((nx,)),
            dma((nx,)),
            dma((2, steps, CHUNKS)),
            dma((2, steps, CHUNKS)),
            dma((nx,)),
            dma((nx,)),
            dma((nx,)),
            dma((nx,)),
            dma((ny,)),
            dma((ny,)),
            dma((ny,)),
            dma((ny,)),
            dma,
            dma,
            dma((nx,)),
            dma((nx,)),
        ],
        compiler_params=pltpu.CompilerParams(
            collective_id=0, has_side_effects=True, vmem_limit_bytes=48 * 1024 * 1024
        ),
        name="experts_backward",
    )(
        tokens,
        cotangent,
        routes.T,
        route_weight.T,
        w_gate[0].T,
        w_up[0].T,
        w_down[0],
    )
    g_tok, g_rw, g_gate, g_up, g_down = outs
    return g_tok.T, g_rw.T, g_gate.T[None], g_up.T[None], g_down[None]


def solution(mesh):
    nz = mesh.shape["ep"] // 2
    nx = 4 if mesh.shape["tp"] >= 16 else 2
    ny = mesh.shape["tp"] // nx
    return jax.shard_map(
        functools.partial(on_device, nz, ny, nx),
        mesh=mesh,
        in_specs=(
            P("ep", None),
            P("ep", None),
            P("ep", None),
            P("ep", None),
            P("ep", None, "tp"),
            P("ep", None, "tp"),
            P("ep", "tp", None),
        ),
        out_specs=(
            P("ep", "tp"),
            P("ep", None),
            P("ep", None, "tp"),
            P("ep", None, "tp"),
            P("ep", "tp", None),
        ),
        check_vma=False,
    )
```

```python
import functools

import jax
import jax.numpy as jnp
from jax import lax
from jax.experimental import pallas as pl
from jax.experimental.pallas import tpu as pltpu
from jax.sharding import PartitionSpec as P

MESH = pl.DeviceIdType.MESH
F32 = jnp.float32
BF16 = jnp.bfloat16
LANES = 128
FEAT = 64
HID = 32
CHUNKS = 4


def dot(a, b, ca, cb):
    return lax.dot_general(a, b, (((ca,), (cb,)), ((), ())), preferred_element_type=F32)


def kernel(
    nz, ny, nx, cap,
    tokens, cotangent, routes_in, weights_in, gate_w, up_w, down_w,
    *refs,
):
    (
        out_hbm0, out_hbm1, out_hbm2, out_hbm3, out_hbm4,
        tok_in, cot_in, gate_in, up_in, down_in, routes, weights,
        onehot0, onehot1, send, rows, w_send, w_all, w_left,
        part_send, part_got, hidden, piece, piece_got, rw_row, rw_got,
        back, back_got, grad_send, grad_got,
        in_sem, z_send, z_recv, w_ssem, w_rsem, ag_ssem, ag_rsem,
        px_ssem, px_rsem, hx_ssem, hx_rsem, ry_ssem, ry_rsem, rw_ssem, rw_rsem,
        b_ssem, b_rsem, g_ssem, g_rsem,
        out_tok, out_rw, out_gate, out_up, out_down, out_sem,
    ) = refs
    nep = 2 * nz
    count = nep * cap
    tok_dev = tokens.shape[0]
    ep = lax.axis_index("ep")
    tp = lax.axis_index("tp")
    z, core = ep // 2, ep % 2
    y, x = tp // nx, tp % nx

    def remote(src, dst, ssem, rsem, to_ep, to_tp):
        return pltpu.make_async_remote_copy(
            src_ref=src, dst_ref=dst, send_sem=ssem, recv_sem=rsem,
            device_id=(to_ep, to_tp), device_id_type=MESH,
        )

    def arrived(ref, sem):
        pltpu.make_async_copy(ref, ref, sem).wait()

    def ep_peer(i, c):
        k = (i + 1) // 2
        dz = nz // 2 + k - 2 * k * (i % 2)
        return ((z + dz) % nz) * 2 + (core + c) % 2

    def x_peer(d):
        return y * nx + (x + d) % nx

    def y_peer(d):
        return ((y + d) % ny) * nx + x

    def col(i):
        return pl.ds(pl.multiple_of(i * LANES, LANES), LANES)

    def slot(e):
        return pl.ds(pl.multiple_of(e * cap, cap), cap)

    barrier = pltpu.get_barrier_semaphore()

    def greet(to_ep, to_tp):
        pl.semaphore_signal(barrier, inc=1, device_id=(to_ep, to_tp), device_id_type=MESH)

    def greet_ep(i, carry):
        greet(ep_peer(i, 0), tp)
        greet(ep_peer(i, 1), tp)
        return carry

    lax.fori_loop(0, nz - 1, greet_ep, 0)
    greet(ep_peer(nz - 1, 1), tp)
    for d in range(1, nx):
        greet(ep, x_peer(d))
    for d in range(1, ny):
        greet(ep, y_peer(d))

    pair = col(tp // 2)
    loads = [
        pltpu.make_async_copy(tokens.at[:, pair], tok_in, in_sem.at[0]),
        pltpu.make_async_copy(cotangent.at[:, pair], cot_in, in_sem.at[1]),
        pltpu.make_async_copy(gate_w, gate_in, in_sem.at[2]),
        pltpu.make_async_copy(up_w, up_in, in_sem.at[3]),
        pltpu.make_async_copy(down_w, down_in, in_sem.at[4]),
        pltpu.make_async_copy(routes_in, routes, in_sem.at[5]),
        pltpu.make_async_copy(weights_in, weights, in_sem.at[6]),
    ]
    for load in loads[5:] + loads[:5]:
        load.start()
    loads[5].wait()
    loads[6].wait()

    ids = lax.broadcasted_iota(jnp.int32, (nep, tok_dev), 0)
    first = (routes[0:1, :] == ids).astype(F32)
    second = (routes[1:2, :] == ids).astype(F32)
    named = first + second
    below = (
        lax.broadcasted_iota(jnp.int32, (tok_dev, tok_dev), 0)
        < lax.broadcasted_iota(jnp.int32, (tok_dev, tok_dev), 1)
    ).astype(F32).astype(BF16)
    place = dot(named.astype(BF16), below, 1, 0)
    at_slot = lax.broadcasted_iota(jnp.int32, (nep, cap, tok_dev), 1).astype(F32)

    def spread(value):
        return jnp.broadcast_to(value[:, None, :], (nep, cap, tok_dev))

    hit = (spread(place) == at_slot).astype(F32)
    hot0 = (hit * spread(first)).reshape(count, tok_dev)
    hot1 = (hit * spread(second)).reshape(count, tok_dev)
    onehot0[...] = hot0.astype(BF16)
    onehot1[...] = hot1.astype(BF16)
    row_w = jnp.sum(hot0 * weights[0:1, :] + hot1 * weights[1:2, :], axis=1, keepdims=True)

    loads[0].wait()
    loads[1].wait()
    lane = lax.broadcasted_iota(jnp.int32, (tok_dev, LANES), 1)
    odd = tp % 2
    tok = tok_in[...].astype(F32)
    cot = cot_in[...].astype(F32)
    tok = jnp.where(odd == 1, pltpu.roll(tok, FEAT, 1), tok)
    cot = jnp.where(odd == 1, cot, pltpu.roll(cot, FEAT, 1))
    both = jnp.where(lane < FEAT, tok, cot).astype(BF16)
    sent = dot((hot0 + hot1).astype(BF16), both, 1, 0)
    row_lane = lax.broadcasted_iota(jnp.int32, (count, LANES), 1)
    send[...] = (sent * jnp.where(row_lane < FEAT, 1.0, row_w)).astype(BF16)

    pl.semaphore_wait(barrier, (nep - 1) + (nx - 1) + (ny - 1))

    group = nep // CHUNKS
    my_group = ep // group

    def dispatch(i, c):
        to = ep_peer(i, c)
        remote(
            send.at[slot(to), :], rows.at[slot(ep), col(y)], z_send, z_recv.at[my_group], to, tp
        ).start()

    def dispatch_both(i, carry):
        dispatch(i, 0)
        dispatch(i, 1)
        return carry

    lax.fori_loop(0, nz - 1, dispatch_both, 0)
    dispatch(nz - 1, 1)
    rows[slot(ep), col(y)] = send[slot(ep), :]

    for load in loads[2:5]:
        load.wait()
    w_lane = lax.broadcasted_iota(jnp.int32, (HID, LANES), 1)
    zero = jnp.zeros((HID, LANES), F32)
    for t in range(nx * ny):
        tile = slice(t // 2 * LANES, (t // 2 + 1) * LANES)
        to_x, to_tile = t % nx, slice(t // nx * LANES, (t // nx + 1) * LANES)
        for k, ref in enumerate((gate_in, up_in, down_in)):
            value = ref[:, tile].astype(F32)
            if (t % 2 == 0) == (k == 2):
                value = pltpu.roll(value, FEAT, 1)
            keep = (w_lane >= FEAT) if k == 2 else (w_lane < FEAT)
            w_send[to_x, k * HID : (k + 1) * HID, to_tile] = jnp.where(keep, value, zero).astype(BF16)
    w_rows = 3 * HID

    def w_place(i):
        return pl.ds(pl.multiple_of(i * LANES, LANES), w_rows)

    w_copies = []
    for d in range(1, nx):
        to = (x + d) % nx
        copy = remote(
            w_send.at[to], w_all.at[w_place(x), :], w_ssem.at[d], w_rsem.at[d], ep, x_peer(d)
        )
        copy.start()
        w_copies.append(copy)
    w_all[w_place(x), :] = w_send[x]
    for i in range(nx):
        w_all[i * LANES + w_rows : (i + 1) * LANES, :] = jnp.zeros((LANES - w_rows, ny * LANES), BF16)

    steps = ny // 2
    per = count // CHUNKS
    pack = per // 2
    order = [0, 1, 3, 2]
    lane_c = lax.broadcasted_iota(jnp.int32, (per, LANES), 1)
    lane_p = lax.broadcasted_iota(jnp.int32, (pack, LANES), 1)
    pick = (lax.broadcasted_iota(jnp.int32, (16, nx * LANES), 1) % LANES == 3 * HID).astype(F32).astype(BF16)
    y_order = [ny // 2 + (k + 1) // 2 * (1 if k % 2 == 0 else -1) for k in range(ny - 1)]
    copies = []

    def launch(copy):
        copy.start()
        copies.append(copy)

    def chunk_of(i):
        return (my_group + order[i]) % CHUNKS

    def chunk_rows(i):
        return pl.ds(pl.multiple_of(chunk_of(i) * per, per), per)

    def ring(way, step, i, owner):
        block = rows.at[chunk_rows(i), col(owner)]
        to = y_peer(1) if way == 0 else y_peer(ny - 1)
        return remote(
            block, block, ag_ssem.at[way, step - 1, i], ag_rsem.at[way, step - 1, i], ep, to
        )

    def owner_of(way, hops):
        return (y + ny - hops) % ny if way == 0 else (y + hops) % ny

    def travels(way, step, i):
        return step < steps or (i < CHUNKS // 2) == (way == 0)

    def gather(i, step):
        if step == 1:
            if order[i] == 0:
                arrived(rows.at[pl.ds(0, per - cap), col(y)], z_recv.at[chunk_of(i)])
            else:
                arrived(rows.at[chunk_rows(i), col(y)], z_recv.at[chunk_of(i)])
        for way in (0, 1):
            if step > 1 and travels(way, step - 1, i):
                ring(way, step - 1, i, owner_of(way, step - 1)).wait_recv()
            if step <= steps and travels(way, step, i):
                launch(ring(way, step, i, owner_of(way, step - 1)))

    def partial(i):
        gather(i, steps + 1)
        if i == 0:
            for d in range(1, nx):
                arrived(w_all.at[w_place((x + nx - d) % nx), :], w_rsem.at[d])
        part_send[i] = dot(rows[chunk_rows(i), :], w_all[...], 1, 1).astype(BF16)
        for d in x_order:
            launch(
                remote(
                    part_send.at[i, :, col((x + d) % nx)], part_got.at[d, i],
                    px_ssem.at[d, i], px_rsem.at[d, i], ep, x_peer(d),
                )
            )
        if i == 0:
            for k in range(nx):
                top = slice(k * LANES, k * LANES + 2 * HID)
                rest = slice(k * LANES + 2 * HID, (k + 1) * LANES)
                w_left[top, :] = w_all[top, :]
                w_left[rest, :] = jnp.zeros((LANES - 2 * HID, ny * LANES), BF16)

    def activate(i):
        pre = part_send[i, :, col(x)].astype(F32)
        for d in range(1, nx):
            arrived(part_got.at[d, i], px_rsem.at[d, i])
            pre = pre + part_got[d, i].astype(F32)
        up = pltpu.roll(pre, LANES - HID, 1)
        d_hidden = pltpu.roll(pre, LANES - 2 * HID, 1)
        sig = jax.nn.sigmoid(pre)
        act = pre * sig * up
        d_gate = d_hidden * up * sig * (1.0 + pre * (1.0 - sig))
        d_up = d_hidden * pre * sig
        rw = jnp.sum(jnp.where(lane_c < HID, act * d_hidden, 0.0), axis=1, keepdims=True)
        tail = jnp.where(lane_c == 3 * HID, rw, 0.0)
        packed = jnp.where(lane_c < 3 * HID, pltpu.roll(act, 2 * HID, 1), tail)
        packed = jnp.where(lane_c < 2 * HID, pltpu.roll(d_up, HID, 1), packed)
        packed = jnp.where(lane_c < HID, d_gate, packed)
        mine = hidden.at[chunk_rows(i), col(x)]
        hidden[chunk_rows(i), col(x)] = packed.astype(BF16)
        for d in x_order:
            launch(remote(mine, mine, hx_ssem.at[d, i], hx_rsem.at[d, i], ep, x_peer(d)))

    def token_part(i):
        for d in range(1, nx):
            arrived(hidden.at[chunk_rows(i), col((x + nx - d) % nx)], hx_rsem.at[d, i])
        value = hidden[chunk_rows(i), :]
        whole = dot(value, w_left[...], 1, 0)
        for j in range(ny):
            tile = slice(j * LANES, (j + 1) * LANES)
            right = pltpu.roll(whole[pack:per, tile], FEAT, 1)
            piece[i, :, tile] = jnp.where(lane_p < FEAT, whole[0:pack, tile], right).astype(BF16)
        rw_row[i] = dot(pick, value, 1, 1)[0:1, :]
        for d in y_order:
            launch(
                remote(
                    piece.at[i, :, col((y + d) % ny)], piece_got.at[d, i],
                    ry_ssem.at[d, i], ry_rsem.at[d, i], ep, y_peer(d),
                )
            )
            launch(
                remote(rw_row.at[i], rw_got.at[d, i], rw_ssem.at[d, i], rw_rsem.at[d, i], ep, y_peer(d))
            )

    def send_back(to):
        remote(back.at[slot(to), :], back_got.at[slot(ep), :], b_ssem, b_rsem, to, tp).start()

    def summed(i):
        total = piece[i, :, col(y)].astype(F32)
        total_rw = rw_row[i]
        for d in y_order[::-1]:
            arrived(piece_got.at[d, i], ry_rsem.at[d, i])
            arrived(rw_got.at[d, i], rw_rsem.at[d, i])
            total = total + piece_got[d, i].astype(F32)
            total_rw = total_rw + rw_got[d, i]
        spread_rw = jnp.broadcast_to(total_rw, (per, per)).T
        both_ = jnp.concatenate([total, pltpu.roll(total, FEAT, 1)], axis=0)
        if per < LANES:
            spread_rw = jnp.broadcast_to(spread_rw[:, 0:1], (per, LANES))
        back[chunk_rows(i), :] = jnp.where(lane_c < FEAT, both_, spread_rw).astype(BF16)
        base = chunk_of(i) * group
        if order[i] == 0:
            back_got[slot(ep), :] = back[slot(ep), :]
        for j in range(1 if order[i] == 0 else 0, group):
            send_back(base + (ep + j) % group)

    x_order = list(range(1, nx))
    stages = [functools.partial(gather, step=s) for s in range(1, steps + 1)]
    stages += [partial, activate, token_part, summed]
    for wave in range(len(stages) + CHUNKS - 1):
        if wave == len(stages) + CHUNKS - 2:
            grads = dot(hidden[...], rows[...], 0, 0)
            g_lane = lax.broadcasted_iota(jnp.int32, (HID, ny * LANES), 1) % LANES
            for k in range(nx):
                at = k * LANES
                gate_down = jnp.where(
                    g_lane < FEAT, grads[at : at + HID, :], grads[at + 2 * HID : at + 3 * HID, :]
                )
                grad_send[k, 0:HID, :] = gate_down.astype(BF16)
                grad_send[k, HID : 2 * HID, :] = grads[at + HID : at + 2 * HID, :].astype(BF16)
            for d in range(1, nx):
                launch(
                    remote(
                        grad_send.at[(x + d) % nx], grad_got.at[x], g_ssem.at[d], g_rsem.at[d],
                        ep, x_peer(d),
                    )
                )
            grad_got[x] = grad_send[x]
        for k, stage in enumerate(stages):
            if 0 <= wave - k < CHUNKS:
                stage(wave - k)

    for d in range(1, nx):
        arrived(grad_got.at[(x + nx - d) % nx], g_rsem.at[d])
    for t in range(0, nx * ny, 2):
        tile = slice(t // 2 * LANES, (t // 2 + 1) * LANES)
        src = slice(t // nx * LANES, (t // nx + 1) * LANES)
        a, b = t % nx, t % nx + 1
        top_a = grad_got[a, 0:HID, src].astype(F32)
        top_b = grad_got[b, 0:HID, src].astype(F32)
        up_a = grad_got[a, HID : 2 * HID, src].astype(F32)
        up_b = grad_got[b, HID : 2 * HID, src].astype(F32)
        out_gate[:, tile] = jnp.where(w_lane < FEAT, top_a, pltpu.roll(top_b, FEAT, 1))
        out_up[:, tile] = jnp.where(w_lane < FEAT, up_a, pltpu.roll(up_b, FEAT, 1))
        out_down[:, tile] = jnp.where(w_lane < FEAT, pltpu.roll(top_a, FEAT, 1), top_b)

    stores = [
        pltpu.make_async_copy(out_tok, out_hbm0, out_sem.at[0]),
        pltpu.make_async_copy(out_rw, out_hbm1, out_sem.at[1]),
        pltpu.make_async_copy(out_gate, out_hbm2, out_sem.at[2]),
        pltpu.make_async_copy(out_up, out_hbm3, out_sem.at[3]),
        pltpu.make_async_copy(out_down, out_hbm4, out_sem.at[4]),
    ]
    for copy in stores[2:]:
        copy.start()
    others = pl.ds(0, (nep - 1) * cap)
    arrived(back_got.at[others, :], b_rsem)
    got = back_got[...]
    by_first = dot(got, onehot0[...], 0, 0)
    by_second = dot(got, onehot1[...], 0, 0)
    out_tok[...] = (by_first[0:FEAT, :] + by_second[0:FEAT, :]).astype(BF16)
    out_rw[0:1, :] = by_first[FEAT : FEAT + 1, :] / weights[0:1, :]
    out_rw[1:2, :] = by_second[FEAT : FEAT + 1, :] / weights[1:2, :]

    for copy in stores[:2]:
        copy.start()
    arrived(send.at[others, :], z_send)
    arrived(back.at[others, :], b_ssem)
    for copy in w_copies + copies:
        copy.wait_send()
    for copy in stores:
        copy.wait()


def store(*refs):
    given, kept, held, sems = refs[0:5], refs[5:10], refs[10:15], refs[15]
    loads = [pltpu.make_async_copy(given[i], held[i], sems.at[0, i]) for i in range(5)]
    stores = [pltpu.make_async_copy(held[i], kept[i], sems.at[1, i]) for i in range(5)]
    for copy in loads:
        copy.start()
    for load, copy in zip(loads, stores):
        load.wait()
        copy.start()
    for copy in stores:
        copy.wait()


def on_device(nz, ny, nx, tokens, cotangent, routes, route_weight, w_gate, w_up, w_down):
    tok_dev, model = tokens.shape
    hid = w_down.shape[1]
    nep = 2 * nz
    cap = 2 * tok_dev * routes.shape[1] // nep
    count = nep * cap
    per = count // CHUNKS
    wide_x, wide_y = nx * LANES, ny * LANES
    steps = ny // 2
    hbm = pl.BlockSpec(memory_space=pltpu.HBM)
    dma = pltpu.SemaphoreType.DMA
    outs = pl.pallas_call(
        functools.partial(kernel, nz, ny, nx, cap),
        out_shape=(
            jax.ShapeDtypeStruct((FEAT, tok_dev), BF16),
            jax.ShapeDtypeStruct((2, tok_dev), F32),
            jax.ShapeDtypeStruct((hid, model), F32),
            jax.ShapeDtypeStruct((hid, model), F32),
            jax.ShapeDtypeStruct((hid, model), F32),
        ),
        in_specs=[hbm] * 7,
        out_specs=[hbm] * 5,
        scratch_shapes=[
            pltpu.VMEM((tok_dev, LANES), BF16),
            pltpu.VMEM((tok_dev, LANES), BF16),
            pltpu.VMEM((hid, model), BF16),
            pltpu.VMEM((hid, model), BF16),
            pltpu.VMEM((hid, model), BF16),
            pltpu.VMEM((2, tok_dev), jnp.int32),
            pltpu.VMEM((2, tok_dev), F32),
            pltpu.VMEM((count, tok_dev), BF16),
            pltpu.VMEM((count, tok_dev), BF16),
            pltpu.VMEM((count, LANES), BF16),
            pltpu.VMEM((count, wide_y), BF16),
            pltpu.VMEM((nx, 3 * HID, wide_y), BF16),
            pltpu.VMEM((wide_x, wide_y), BF16),
            pltpu.VMEM((wide_x, wide_y), BF16),
            pltpu.VMEM((CHUNKS, per, wide_x), BF16),
            pltpu.VMEM((nx, CHUNKS, per, LANES), BF16),
            pltpu.VMEM((count, wide_x), BF16),
            pltpu.VMEM((CHUNKS, per // 2, wide_y), BF16),
            pltpu.VMEM((ny, CHUNKS, per // 2, LANES), BF16),
            pltpu.VMEM((CHUNKS, 1, per), F32),
            pltpu.VMEM((ny, CHUNKS, 1, per), F32),
            pltpu.VMEM((count, LANES), BF16),
            pltpu.VMEM((count, LANES), BF16),
            pltpu.VMEM((nx, 2 * HID, wide_y), BF16),
            pltpu.VMEM((nx, 2 * HID, wide_y), BF16),
            dma((7,)),
            dma,
            dma((CHUNKS,)),
            dma((nx,)),
            dma((nx,)),
            dma((2, steps, CHUNKS)),
            dma((2, steps, CHUNKS)),
            dma((nx, CHUNKS)),
            dma((nx, CHUNKS)),
            dma((nx, CHUNKS)),
            dma((nx, CHUNKS)),
            dma((ny, CHUNKS)),
            dma((ny, CHUNKS)),
            dma((ny, CHUNKS)),
            dma((ny, CHUNKS)),
            dma,
            dma,
            dma((nx,)),
            dma((nx,)),
            pltpu.VMEM((FEAT, tok_dev), BF16),
            pltpu.VMEM((2, tok_dev), F32),
            pltpu.VMEM((hid, model), F32),
            pltpu.VMEM((hid, model), F32),
            pltpu.VMEM((hid, model), F32),
            dma((5,)),
        ],
        compiler_params=pltpu.CompilerParams(
            collective_id=0, has_side_effects=True, vmem_limit_bytes=62 * 1024 * 1024
        ),
        name="experts_backward",
    )(
        tokens,
        cotangent,
        routes.T,
        route_weight.T,
        w_gate[0].T,
        w_up[0].T,
        w_down[0],
    )
    g_tok, g_rw, g_gate, g_up, g_down = pl.pallas_call(
        store,
        out_shape=tuple(jax.ShapeDtypeStruct(o.shape, o.dtype) for o in outs),
        in_specs=[hbm] * 5,
        out_specs=[hbm] * 5,
        scratch_shapes=[pltpu.VMEM(o.shape, o.dtype) for o in outs] + [dma((2, 5))],
        compiler_params=pltpu.CompilerParams(vmem_limit_bytes=62 * 1024 * 1024),
        name="store",
    )(*outs)
    return g_tok.T, g_rw.T, g_gate.T[None], g_up.T[None], g_down[None]


def solution(mesh):
    nz = mesh.shape["ep"] // 2
    nx = 4 if mesh.shape["tp"] >= 16 else 2
    ny = mesh.shape["tp"] // nx
    return jax.shard_map(
        functools.partial(on_device, nz, ny, nx),
        mesh=mesh,
        in_specs=(
            P("ep", None),
            P("ep", None),
            P("ep", None),
            P("ep", None),
            P("ep", None, "tp"),
            P("ep", None, "tp"),
            P("ep", "tp", None),
        ),
        out_specs=(
            P("ep", "tp"),
            P("ep", None),
            P("ep", None, "tp"),
            P("ep", None, "tp"),
            P("ep", "tp", None),
        ),
        check_vma=False,
    )
```

```python
import functools

import jax
import jax.numpy as jnp
from jax import lax
from jax.experimental import pallas as pl
from jax.experimental.pallas import tpu as pltpu
from jax.sharding import PartitionSpec as P

MESH = pl.DeviceIdType.MESH
F32 = jnp.float32
BF16 = jnp.bfloat16
LANES = 128
FEAT = 64
HID = 32
CHUNKS = 4


def dot(a, b, ca, cb):
    return lax.dot_general(a, b, (((ca,), (cb,)), ((), ())), preferred_element_type=F32)


def kernel(
    nz, ny, nx, cap,
    tokens, cotangent, routes_in, weights_in, gate_w, up_w, down_w,
    *refs,
):
    (
        out_hbm0, out_hbm1, out_hbm2, out_hbm3, out_hbm4,
        tok_in, cot_in, gate_in, up_in, down_in, routes, weights,
        onehot0, onehot1, send, rows, w_send, w_all, w_left,
        part_send, part_got, hidden, piece, piece_got, rw_row, rw_got,
        back, back_got, grad_send, grad_got,
        in_sem, z_send, z_recv, w_ssem, w_rsem, ag_ssem, ag_rsem,
        px_ssem, px_rsem, hx_ssem, hx_rsem, ry_ssem, ry_rsem, rw_ssem, rw_rsem,
        b_ssem, b_rsem, g_ssem, g_rsem,
        out_tok, out_rw, out_gate, out_up, out_down, out_sem,
    ) = refs
    nep = 2 * nz
    count = nep * cap
    tok_dev = tokens.shape[0]
    ep = lax.axis_index("ep")
    tp = lax.axis_index("tp")
    z, core = ep // 2, ep % 2
    y, x = tp // nx, tp % nx

    def remote(src, dst, ssem, rsem, to_ep, to_tp):
        return pltpu.make_async_remote_copy(
            src_ref=src, dst_ref=dst, send_sem=ssem, recv_sem=rsem,
            device_id=(to_ep, to_tp), device_id_type=MESH,
        )

    def arrived(ref, sem):
        pltpu.make_async_copy(ref, ref, sem).wait()

    def ep_peer(i, c):
        k = (i + 1) // 2
        dz = nz // 2 + k - 2 * k * (i % 2)
        return ((z + dz) % nz) * 2 + (core + c) % 2

    def x_peer(d):
        return y * nx + (x + d) % nx

    def y_peer(d):
        return ((y + d) % ny) * nx + x

    def col(i):
        return pl.ds(pl.multiple_of(i * LANES, LANES), LANES)

    def slot(e):
        return pl.ds(pl.multiple_of(e * cap, cap), cap)

    barrier = pltpu.get_barrier_semaphore()

    def greet(to_ep, to_tp):
        pl.semaphore_signal(barrier, inc=1, device_id=(to_ep, to_tp), device_id_type=MESH)

    def greet_ep(i, carry):
        greet(ep_peer(i, 0), tp)
        greet(ep_peer(i, 1), tp)
        return carry

    lax.fori_loop(0, nz - 1, greet_ep, 0)
    greet(ep_peer(nz - 1, 1), tp)
    for d in range(1, nx):
        greet(ep, x_peer(d))
    for d in range(1, ny):
        greet(ep, y_peer(d))

    pair = col(tp // 2)
    loads = [
        pltpu.make_async_copy(tokens.at[:, pair], tok_in, in_sem.at[0]),
        pltpu.make_async_copy(cotangent.at[:, pair], cot_in, in_sem.at[1]),
        pltpu.make_async_copy(gate_w, gate_in, in_sem.at[2]),
        pltpu.make_async_copy(up_w, up_in, in_sem.at[3]),
        pltpu.make_async_copy(down_w, down_in, in_sem.at[4]),
        pltpu.make_async_copy(routes_in, routes, in_sem.at[5]),
        pltpu.make_async_copy(weights_in, weights, in_sem.at[6]),
    ]
    for load in loads[5:] + loads[:5]:
        load.start()
    loads[5].wait()
    loads[6].wait()

    ids = lax.broadcasted_iota(jnp.int32, (nep, tok_dev), 0)
    first = (routes[0:1, :] == ids).astype(F32)
    second = (routes[1:2, :] == ids).astype(F32)
    named = first + second
    below = (
        lax.broadcasted_iota(jnp.int32, (tok_dev, tok_dev), 0)
        < lax.broadcasted_iota(jnp.int32, (tok_dev, tok_dev), 1)
    ).astype(F32).astype(BF16)
    place = dot(named.astype(BF16), below, 1, 0)
    at_slot = lax.broadcasted_iota(jnp.int32, (nep, cap, tok_dev), 1).astype(F32)

    def spread(value):
        return jnp.broadcast_to(value[:, None, :], (nep, cap, tok_dev))

    hit = (spread(place) == at_slot).astype(F32)
    hot0 = (hit * spread(first)).reshape(count, tok_dev)
    hot1 = (hit * spread(second)).reshape(count, tok_dev)
    onehot0[...] = hot0.astype(BF16)
    onehot1[...] = hot1.astype(BF16)
    row_w = jnp.sum(hot0 * weights[0:1, :] + hot1 * weights[1:2, :], axis=1, keepdims=True)

    loads[0].wait()
    loads[1].wait()
    lane = lax.broadcasted_iota(jnp.int32, (tok_dev, LANES), 1)
    odd = tp % 2
    tok = tok_in[...].astype(F32)
    cot = cot_in[...].astype(F32)
    tok = jnp.where(odd == 1, pltpu.roll(tok, FEAT, 1), tok)
    cot = jnp.where(odd == 1, cot, pltpu.roll(cot, FEAT, 1))
    both = jnp.where(lane < FEAT, tok, cot).astype(BF16)
    sent = dot((hot0 + hot1).astype(BF16), both, 1, 0)
    row_lane = lax.broadcasted_iota(jnp.int32, (count, LANES), 1)
    send[...] = (sent * jnp.where(row_lane < FEAT, 1.0, row_w)).astype(BF16)

    pl.semaphore_wait(barrier, (nep - 1) + (nx - 1) + (ny - 1))

    group = nep // CHUNKS
    my_group = ep // group

    def dispatch(i, c):
        to = ep_peer(i, c)
        remote(
            send.at[slot(to), :], rows.at[slot(ep), col(y)], z_send, z_recv.at[my_group], to, tp
        ).start()

    def dispatch_both(i, carry):
        dispatch(i, 0)
        dispatch(i, 1)
        return carry

    lax.fori_loop(0, nz - 1, dispatch_both, 0)
    dispatch(nz - 1, 1)
    rows[slot(ep), col(y)] = send[slot(ep), :]

    for load in loads[2:5]:
        load.wait()
    w_lane = lax.broadcasted_iota(jnp.int32, (HID, LANES), 1)
    zero = jnp.zeros((HID, LANES), F32)
    for t in range(nx * ny):
        tile = slice(t // 2 * LANES, (t // 2 + 1) * LANES)
        to_x, to_tile = t % nx, slice(t // nx * LANES, (t // nx + 1) * LANES)
        for k, ref in enumerate((gate_in, up_in, down_in)):
            value = ref[:, tile].astype(F32)
            if (t % 2 == 0) == (k == 2):
                value = pltpu.roll(value, FEAT, 1)
            keep = (w_lane >= FEAT) if k == 2 else (w_lane < FEAT)
            w_send[to_x, k * HID : (k + 1) * HID, to_tile] = jnp.where(keep, value, zero).astype(BF16)
    w_rows = 3 * HID

    def w_place(i):
        return pl.ds(pl.multiple_of(i * LANES, LANES), w_rows)

    w_copies = []
    for d in range(1, nx):
        to = (x + d) % nx
        copy = remote(
            w_send.at[to], w_all.at[w_place(x), :], w_ssem.at[d], w_rsem.at[d], ep, x_peer(d)
        )
        copy.start()
        w_copies.append(copy)
    w_all[w_place(x), :] = w_send[x]
    for i in range(nx):
        w_all[i * LANES + w_rows : (i + 1) * LANES, :] = jnp.zeros((LANES - w_rows, ny * LANES), BF16)

    steps = ny // 2
    per = count // CHUNKS
    pack = per // 2
    order = [2, 1, 3, 0]
    copies_wide = LANES // per
    lane_c = lax.broadcasted_iota(jnp.int32, (per, LANES), 1)
    lane_p = lax.broadcasted_iota(jnp.int32, (pack, LANES), 1)
    pick = (lax.broadcasted_iota(jnp.int32, (16, nx * LANES), 1) % LANES == 3 * HID).astype(F32).astype(BF16)
    y_order = [ny // 2 + (k + 1) // 2 * (1 if k % 2 == 0 else -1) for k in range(ny - 1)]
    copies = []

    def launch(copy):
        copy.start()
        copies.append(copy)

    def chunk_of(i):
        return (my_group + order[i]) % CHUNKS

    def chunk_rows(i):
        return pl.ds(pl.multiple_of(chunk_of(i) * per, per), per)

    def toward(way, hops):
        return (y + hops) % ny if way == 0 else (y + ny - hops) % ny

    def reach(way, hops, i):
        step, owner = (hops, y) if hops <= 2 else (hops - 2, toward(1 - way, 2))
        block = rows.at[chunk_rows(i), col(owner)]
        return remote(
            block, block, ag_ssem.at[way, hops - 1, i], ag_rsem.at[way, hops - 1, i],
            ep, toward(way, step) * nx + x,
        )

    def reached(way, hops, i):
        arrived(rows.at[chunk_rows(i), col(toward(1 - way, hops))], ag_rsem.at[way, hops - 1, i])

    def travels(way, hops, i):
        return hops < steps or (i < CHUNKS // 2) == (way == 0)

    def spread_near(i):
        if order[i] == 0:
            arrived(rows.at[pl.ds(0, per - cap), col(y)], z_recv.at[chunk_of(i)])
        else:
            arrived(rows.at[chunk_rows(i), col(y)], z_recv.at[chunk_of(i)])
        for hops in (2, 1):
            for way in (0, 1):
                launch(reach(way, hops, i))

    def spread_far(i):
        for way in (0, 1):
            reached(way, 2, i)
            for hops in (4, 3):
                if travels(way, hops, i):
                    launch(reach(way, hops, i))

    def partial(i):
        for hops in (1, 3, 4):
            for way in (0, 1):
                if travels(way, hops, i):
                    reached(way, hops, i)
        if i == 0:
            for d in range(1, nx):
                arrived(w_all.at[w_place((x + nx - d) % nx), :], w_rsem.at[d])
        part_send[i] = dot(rows[chunk_rows(i), :], w_all[...], 1, 1).astype(BF16)
        for d in x_order:
            launch(
                remote(
                    part_send.at[i, :, col((x + d) % nx)], part_got.at[d, i],
                    px_ssem.at[d, i], px_rsem.at[d, i], ep, x_peer(d),
                )
            )
        if i == 0:
            for k in range(nx):
                top = slice(k * LANES, k * LANES + 2 * HID)
                rest = slice(k * LANES + 2 * HID, (k + 1) * LANES)
                w_left[top, :] = w_all[top, :]
                w_left[rest, :] = jnp.zeros((LANES - 2 * HID, ny * LANES), BF16)

    def activate(i):
        pre = part_send[i, :, col(x)].astype(F32)
        for d in range(1, nx):
            arrived(part_got.at[d, i], px_rsem.at[d, i])
            pre = pre + part_got[d, i].astype(F32)
        up = pltpu.roll(pre, LANES - HID, 1)
        d_hidden = pltpu.roll(pre, LANES - 2 * HID, 1)
        sig = jax.nn.sigmoid(pre)
        act = pre * sig * up
        d_gate = d_hidden * up * sig * (1.0 + pre * (1.0 - sig))
        d_up = d_hidden * pre * sig
        rw = jnp.sum(jnp.where(lane_c < HID, act * d_hidden, 0.0), axis=1, keepdims=True)
        tail = jnp.where(lane_c == 3 * HID, rw, 0.0)
        packed = jnp.where(lane_c < 3 * HID, pltpu.roll(act, 2 * HID, 1), tail)
        packed = jnp.where(lane_c < 2 * HID, pltpu.roll(d_up, HID, 1), packed)
        packed = jnp.where(lane_c < HID, d_gate, packed)
        mine = hidden.at[chunk_rows(i), col(x)]
        hidden[chunk_rows(i), col(x)] = packed.astype(BF16)
        for d in x_order:
            launch(remote(mine, mine, hx_ssem.at[d, i], hx_rsem.at[d, i], ep, x_peer(d)))

    def token_part(i):
        for d in range(1, nx):
            arrived(hidden.at[chunk_rows(i), col((x + nx - d) % nx)], hx_rsem.at[d, i])
        value = hidden[chunk_rows(i), :]
        whole = dot(value, w_left[...], 1, 0)
        for j in range(ny):
            tile = slice(j * LANES, (j + 1) * LANES)
            right = pltpu.roll(whole[pack:per, tile], FEAT, 1)
            piece[i, :, tile] = jnp.where(lane_p < FEAT, whole[0:pack, tile], right).astype(BF16)
        rw_row[i] = jnp.concatenate([dot(pick, value, 1, 1)[0:1, :]] * copies_wide, axis=1)
        for d in y_order:
            launch(
                remote(
                    piece.at[i, :, col((y + d) % ny)], piece_got.at[d, i],
                    ry_ssem.at[d, i], ry_rsem.at[d, i], ep, y_peer(d),
                )
            )
            launch(
                remote(rw_row.at[i], rw_got.at[d, i], rw_ssem.at[d, i], rw_rsem.at[d, i], ep, y_peer(d))
            )

    def send_back(to):
        remote(back.at[slot(to), :], back_got.at[slot(ep), :], b_ssem, b_rsem, to, tp).start()

    def summed(i):
        total = piece[i, :, col(y)].astype(F32)
        total_rw = rw_row[i]
        for d in y_order[::-1]:
            arrived(piece_got.at[d, i], ry_rsem.at[d, i])
            arrived(rw_got.at[d, i], rw_rsem.at[d, i])
            total = total + piece_got[d, i].astype(F32)
            total_rw = total_rw + rw_got[d, i]
        spread_rw = jnp.broadcast_to(total_rw, (LANES, LANES)).T[0:per, :]
        both_ = jnp.concatenate([total, pltpu.roll(total, FEAT, 1)], axis=0)
        back[chunk_rows(i), :] = jnp.where(lane_c < FEAT, both_, spread_rw).astype(BF16)
        base = chunk_of(i) * group
        if order[i] == 0:
            back_got[slot(ep), :] = back[slot(ep), :]
        for j in range(1 if order[i] == 0 else 0, group):
            send_back(base + (ep + j) % group)

    x_order = list(range(1, nx))
    stages = [spread_near, spread_far, partial, activate, token_part, summed]
    after = [0, 4, 8, 13, 18, 26]
    turns = sorted(
        (after[k] + 3 * i, k, i) for k in range(len(stages)) for i in range(CHUNKS)
    )
    for _, k, i in turns:
        if (k, i) == (len(stages) - 1, CHUNKS - 1):
            grads = dot(hidden[...], rows[...], 0, 0)
            g_lane = lax.broadcasted_iota(jnp.int32, (HID, ny * LANES), 1) % LANES
            for n in range(nx):
                at = n * LANES
                gate_down = jnp.where(
                    g_lane < FEAT, grads[at : at + HID, :], grads[at + 2 * HID : at + 3 * HID, :]
                )
                grad_send[n, 0:HID, :] = gate_down.astype(BF16)
                grad_send[n, HID : 2 * HID, :] = grads[at + HID : at + 2 * HID, :].astype(BF16)
            for d in range(1, nx):
                launch(
                    remote(
                        grad_send.at[(x + d) % nx], grad_got.at[x], g_ssem.at[d], g_rsem.at[d],
                        ep, x_peer(d),
                    )
                )
            grad_got[x] = grad_send[x]
        stages[k](i)

    for d in range(1, nx):
        arrived(grad_got.at[(x + nx - d) % nx], g_rsem.at[d])
    for t in range(0, nx * ny, 2):
        tile = slice(t // 2 * LANES, (t // 2 + 1) * LANES)
        src = slice(t // nx * LANES, (t // nx + 1) * LANES)
        a, b = t % nx, t % nx + 1
        top_a = grad_got[a, 0:HID, src].astype(F32)
        top_b = grad_got[b, 0:HID, src].astype(F32)
        up_a = grad_got[a, HID : 2 * HID, src].astype(F32)
        up_b = grad_got[b, HID : 2 * HID, src].astype(F32)
        out_gate[:, tile] = jnp.where(w_lane < FEAT, top_a, pltpu.roll(top_b, FEAT, 1))
        out_up[:, tile] = jnp.where(w_lane < FEAT, up_a, pltpu.roll(up_b, FEAT, 1))
        out_down[:, tile] = jnp.where(w_lane < FEAT, pltpu.roll(top_a, FEAT, 1), top_b)

    stores = [
        pltpu.make_async_copy(out_tok, out_hbm0, out_sem.at[0]),
        pltpu.make_async_copy(out_rw, out_hbm1, out_sem.at[1]),
        pltpu.make_async_copy(out_gate, out_hbm2, out_sem.at[2]),
        pltpu.make_async_copy(out_up, out_hbm3, out_sem.at[3]),
        pltpu.make_async_copy(out_down, out_hbm4, out_sem.at[4]),
    ]
    for copy in stores[2:]:
        copy.start()
    others = pl.ds(0, (nep - 1) * cap)
    arrived(back_got.at[others, :], b_rsem)
    got = back_got[...]
    by_first = dot(got, onehot0[...], 0, 0)
    by_second = dot(got, onehot1[...], 0, 0)
    out_tok[...] = (by_first[0:FEAT, :] + by_second[0:FEAT, :]).astype(BF16)
    out_rw[0:1, :] = by_first[FEAT : FEAT + 1, :] / weights[0:1, :]
    out_rw[1:2, :] = by_second[FEAT : FEAT + 1, :] / weights[1:2, :]

    for copy in stores[:2]:
        copy.start()
    arrived(send.at[others, :], z_send)
    arrived(back.at[others, :], b_ssem)
    for copy in w_copies + copies:
        copy.wait_send()
    for copy in stores:
        copy.wait()


def store(*refs):
    given, kept, held, sems = refs[0:5], refs[5:10], refs[10:15], refs[15]
    loads = [pltpu.make_async_copy(given[i], held[i], sems.at[0, i]) for i in range(5)]
    stores = [pltpu.make_async_copy(held[i], kept[i], sems.at[1, i]) for i in range(5)]
    for copy in loads:
        copy.start()
    for load, copy in zip(loads, stores):
        load.wait()
        copy.start()
    for copy in stores:
        copy.wait()


def on_device(nz, ny, nx, tokens, cotangent, routes, route_weight, w_gate, w_up, w_down):
    tok_dev, model = tokens.shape
    hid = w_down.shape[1]
    nep = 2 * nz
    cap = 2 * tok_dev * routes.shape[1] // nep
    count = nep * cap
    per = count // CHUNKS
    wide_x, wide_y = nx * LANES, ny * LANES
    steps = ny // 2
    hbm = pl.BlockSpec(memory_space=pltpu.HBM)
    dma = pltpu.SemaphoreType.DMA
    outs = pl.pallas_call(
        functools.partial(kernel, nz, ny, nx, cap),
        out_shape=(
            jax.ShapeDtypeStruct((FEAT, tok_dev), BF16),
            jax.ShapeDtypeStruct((2, tok_dev), F32),
            jax.ShapeDtypeStruct((hid, model), F32),
            jax.ShapeDtypeStruct((hid, model), F32),
            jax.ShapeDtypeStruct((hid, model), F32),
        ),
        in_specs=[hbm] * 7,
        out_specs=[hbm] * 5,
        scratch_shapes=[
            pltpu.VMEM((tok_dev, LANES), BF16),
            pltpu.VMEM((tok_dev, LANES), BF16),
            pltpu.VMEM((hid, model), BF16),
            pltpu.VMEM((hid, model), BF16),
            pltpu.VMEM((hid, model), BF16),
            pltpu.VMEM((2, tok_dev), jnp.int32),
            pltpu.VMEM((2, tok_dev), F32),
            pltpu.VMEM((count, tok_dev), BF16),
            pltpu.VMEM((count, tok_dev), BF16),
            pltpu.VMEM((count, LANES), BF16),
            pltpu.VMEM((count, wide_y), BF16),
            pltpu.VMEM((nx, 3 * HID, wide_y), BF16),
            pltpu.VMEM((wide_x, wide_y), BF16),
            pltpu.VMEM((wide_x, wide_y), BF16),
            pltpu.VMEM((CHUNKS, per, wide_x), BF16),
            pltpu.VMEM((nx, CHUNKS, per, LANES), BF16),
            pltpu.VMEM((count, wide_x), BF16),
            pltpu.VMEM((CHUNKS, per // 2, wide_y), BF16),
            pltpu.VMEM((ny, CHUNKS, per // 2, LANES), BF16),
            pltpu.VMEM((CHUNKS, 1, LANES), F32),
            pltpu.VMEM((ny, CHUNKS, 1, LANES), F32),
            pltpu.VMEM((count, LANES), BF16),
            pltpu.VMEM((count, LANES), BF16),
            pltpu.VMEM((nx, 2 * HID, wide_y), BF16),
            pltpu.VMEM((nx, 2 * HID, wide_y), BF16),
            dma((7,)),
            dma,
            dma((CHUNKS,)),
            dma((nx,)),
            dma((nx,)),
            dma((2, steps, CHUNKS)),
            dma((2, steps, CHUNKS)),
            dma((nx, CHUNKS)),
            dma((nx, CHUNKS)),
            dma((nx, CHUNKS)),
            dma((nx, CHUNKS)),
            dma((ny, CHUNKS)),
            dma((ny, CHUNKS)),
            dma((ny, CHUNKS)),
            dma((ny, CHUNKS)),
            dma,
            dma,
            dma((nx,)),
            dma((nx,)),
            pltpu.VMEM((FEAT, tok_dev), BF16),
            pltpu.VMEM((2, tok_dev), F32),
            pltpu.VMEM((hid, model), F32),
            pltpu.VMEM((hid, model), F32),
            pltpu.VMEM((hid, model), F32),
            dma((5,)),
        ],
        compiler_params=pltpu.CompilerParams(
            collective_id=0, has_side_effects=True, vmem_limit_bytes=62 * 1024 * 1024
        ),
        name="experts_backward",
    )(
        tokens,
        cotangent,
        routes.T,
        route_weight.T,
        w_gate[0].T,
        w_up[0].T,
        w_down[0],
    )
    g_tok, g_rw, g_gate, g_up, g_down = pl.pallas_call(
        store,
        out_shape=tuple(jax.ShapeDtypeStruct(o.shape, o.dtype) for o in outs),
        in_specs=[hbm] * 5,
        out_specs=[hbm] * 5,
        scratch_shapes=[pltpu.VMEM(o.shape, o.dtype) for o in outs] + [dma((2, 5))],
        compiler_params=pltpu.CompilerParams(vmem_limit_bytes=62 * 1024 * 1024),
        name="store",
    )(*outs)
    return g_tok.T, g_rw.T, g_gate.T[None], g_up.T[None], g_down[None]


def solution(mesh):
    nz = mesh.shape["ep"] // 2
    nx = 4 if mesh.shape["tp"] >= 16 else 2
    ny = mesh.shape["tp"] // nx
    return jax.shard_map(
        functools.partial(on_device, nz, ny, nx),
        mesh=mesh,
        in_specs=(
            P("ep", None),
            P("ep", None),
            P("ep", None),
            P("ep", None),
            P("ep", None, "tp"),
            P("ep", None, "tp"),
            P("ep", "tp", None),
        ),
        out_specs=(
            P("ep", "tp"),
            P("ep", None),
            P("ep", None, "tp"),
            P("ep", None, "tp"),
            P("ep", "tp", None),
        ),
        check_vma=False,
    )
```

```python
import functools

import jax
import jax.numpy as jnp
from jax import lax
from jax.experimental import pallas as pl
from jax.experimental.pallas import tpu as pltpu
from jax.sharding import PartitionSpec as P

MESH = pl.DeviceIdType.MESH
F32 = jnp.float32
BF16 = jnp.bfloat16
LANES = 128
FEAT = 64
HID = 32
CHUNKS = 4


def dot(a, b, ca, cb):
    return lax.dot_general(a, b, (((ca,), (cb,)), ((), ())), preferred_element_type=F32)


def kernel(
    nz, ny, nx, cap,
    tokens, cotangent, routes_in, weights_in, gate_w, up_w, down_w,
    *refs,
):
    (
        out_hbm0, out_hbm1, out_hbm2, out_hbm3, out_hbm4,
        tok_in, cot_in, gate_in, up_in, down_in, routes, weights,
        onehot0, onehot1, send, rows, w_send, w_all, w_left,
        part_send, part_got, hidden, piece, piece_got, rw_row, rw_got,
        back, back_got, grad_send, grad_got,
        in_sem, z_send, z_recv, w_ssem, w_rsem, ag_ssem, ag_rsem,
        px_ssem, px_rsem, hx_ssem, hx_rsem, ry_ssem, ry_rsem, rw_ssem, rw_rsem,
        b_ssem, b_rsem, g_ssem, g_rsem,
        out_tok, out_rw, out_gate, out_up, out_down, out_sem,
    ) = refs
    nep = 2 * nz
    count = nep * cap
    tok_dev = tokens.shape[0]
    ep = lax.axis_index("ep")
    tp = lax.axis_index("tp")
    z, core = ep // 2, ep % 2
    y, x = tp // nx, tp % nx

    def remote(src, dst, ssem, rsem, to_ep, to_tp):
        return pltpu.make_async_remote_copy(
            src_ref=src, dst_ref=dst, send_sem=ssem, recv_sem=rsem,
            device_id=(to_ep, to_tp), device_id_type=MESH,
        )

    def arrived(ref, sem):
        pltpu.make_async_copy(ref, ref, sem).wait()

    def ep_peer(i, c):
        k = (i + 1) // 2
        dz = nz // 2 + k - 2 * k * (i % 2)
        return ((z + dz) % nz) * 2 + (core + c) % 2

    def x_peer(d):
        return y * nx + (x + d) % nx

    def y_peer(d):
        return ((y + d) % ny) * nx + x

    def col(i):
        return pl.ds(pl.multiple_of(i * LANES, LANES), LANES)

    def slot(e):
        return pl.ds(pl.multiple_of(e * cap, cap), cap)

    pair = col(tp // 2)
    loads = [
        pltpu.make_async_copy(tokens.at[:, pair], tok_in, in_sem.at[0]),
        pltpu.make_async_copy(cotangent.at[:, pair], cot_in, in_sem.at[1]),
        pltpu.make_async_copy(gate_w, gate_in, in_sem.at[2]),
        pltpu.make_async_copy(up_w, up_in, in_sem.at[3]),
        pltpu.make_async_copy(down_w, down_in, in_sem.at[4]),
        pltpu.make_async_copy(routes_in, routes, in_sem.at[5]),
        pltpu.make_async_copy(weights_in, weights, in_sem.at[6]),
    ]
    for load in loads[5:] + loads[:5]:
        load.start()
    barrier = pltpu.get_barrier_semaphore()

    def greet(to_ep, to_tp):
        pl.semaphore_signal(barrier, inc=1, device_id=(to_ep, to_tp), device_id_type=MESH)

    def greet_ep(i, carry):
        greet(ep_peer(i, 0), tp)
        greet(ep_peer(i, 1), tp)
        return carry

    lax.fori_loop(0, nz - 1, greet_ep, 0)
    greet(ep_peer(nz - 1, 1), tp)
    for d in range(1, nx):
        greet(ep, x_peer(d))
    for d in range(1, ny):
        greet(ep, y_peer(d))

    loads[5].wait()
    loads[6].wait()

    ids = lax.broadcasted_iota(jnp.int32, (nep, tok_dev), 0)
    first = (routes[0:1, :] == ids).astype(F32)
    second = (routes[1:2, :] == ids).astype(F32)
    named = first + second
    below = (
        lax.broadcasted_iota(jnp.int32, (tok_dev, tok_dev), 0)
        < lax.broadcasted_iota(jnp.int32, (tok_dev, tok_dev), 1)
    ).astype(F32).astype(BF16)
    place = dot(named.astype(BF16), below, 1, 0)
    at_slot = lax.broadcasted_iota(jnp.int32, (nep, cap, tok_dev), 1).astype(F32)

    def spread(value):
        return jnp.broadcast_to(value[:, None, :], (nep, cap, tok_dev))

    hit = (spread(place) == at_slot).astype(F32)
    hot0 = (hit * spread(first)).reshape(count, tok_dev)
    hot1 = (hit * spread(second)).reshape(count, tok_dev)
    onehot0[...] = hot0.astype(BF16)
    onehot1[...] = hot1.astype(BF16)
    row_w = jnp.sum(hot0 * weights[0:1, :] + hot1 * weights[1:2, :], axis=1, keepdims=True)

    loads[0].wait()
    loads[1].wait()
    lane = lax.broadcasted_iota(jnp.int32, (tok_dev, LANES), 1)
    odd = tp % 2
    tok = tok_in[...].astype(F32)
    cot = cot_in[...].astype(F32)
    tok = jnp.where(odd == 1, pltpu.roll(tok, FEAT, 1), tok)
    cot = jnp.where(odd == 1, cot, pltpu.roll(cot, FEAT, 1))
    both = jnp.where(lane < FEAT, tok, cot).astype(BF16)
    sent = dot((hot0 + hot1).astype(BF16), both, 1, 0)
    row_lane = lax.broadcasted_iota(jnp.int32, (count, LANES), 1)
    send[...] = (sent * jnp.where(row_lane < FEAT, 1.0, row_w)).astype(BF16)

    pl.semaphore_wait(barrier, (nep - 1) + (nx - 1) + (ny - 1))

    group = nep // CHUNKS
    my_group = ep // group

    def dispatch(i, c):
        to = ep_peer(i, c)
        remote(
            send.at[slot(to), :], rows.at[slot(ep), col(y)], z_send, z_recv.at[my_group], to, tp
        ).start()

    def dispatch_both(i, carry):
        dispatch(i, 0)
        dispatch(i, 1)
        return carry

    lax.fori_loop(0, nz - 1, dispatch_both, 0)
    dispatch(nz - 1, 1)
    rows[slot(ep), col(y)] = send[slot(ep), :]

    for load in loads[2:5]:
        load.wait()
    w_lane = lax.broadcasted_iota(jnp.int32, (HID, LANES), 1)
    zero = jnp.zeros((HID, LANES), F32)
    for t in range(nx * ny):
        tile = slice(t // 2 * LANES, (t // 2 + 1) * LANES)
        to_x, to_tile = t % nx, slice(t // nx * LANES, (t // nx + 1) * LANES)
        for k, ref in enumerate((gate_in, up_in, down_in)):
            value = ref[:, tile].astype(F32)
            if (t % 2 == 0) == (k == 2):
                value = pltpu.roll(value, FEAT, 1)
            keep = (w_lane >= FEAT) if k == 2 else (w_lane < FEAT)
            w_send[to_x, k * HID : (k + 1) * HID, to_tile] = jnp.where(keep, value, zero).astype(BF16)
    w_rows = 3 * HID

    def w_place(i):
        return pl.ds(pl.multiple_of(i * LANES, LANES), w_rows)

    w_copies = []
    for d in range(1, nx):
        to = (x + d) % nx
        copy = remote(
            w_send.at[to], w_all.at[w_place(x), :], w_ssem.at[d], w_rsem.at[d], ep, x_peer(d)
        )
        copy.start()
        w_copies.append(copy)
    w_all[w_place(x), :] = w_send[x]
    for i in range(nx):
        w_all[i * LANES + w_rows : (i + 1) * LANES, :] = jnp.zeros((LANES - w_rows, ny * LANES), BF16)

    steps = ny // 2
    per = count // CHUNKS
    pack = per // 2
    order = [2, 1, 3, 0]
    copies_wide = LANES // per
    lane_c = lax.broadcasted_iota(jnp.int32, (per, LANES), 1)
    lane_p = lax.broadcasted_iota(jnp.int32, (pack, LANES), 1)
    pick = (lax.broadcasted_iota(jnp.int32, (16, nx * LANES), 1) % LANES == 3 * HID).astype(F32).astype(BF16)
    y_order = [ny // 2 + (k + 1) // 2 * (1 if k % 2 == 0 else -1) for k in range(ny - 1)]
    copies = []
    x_order = sorted(range(1, nx), key=lambda d: -min(d, nx - d))

    def launch(copy):
        copy.start()
        copies.append(copy)

    def chunk_of(i):
        return (my_group + order[i]) % CHUNKS

    def chunk_rows(i):
        return pl.ds(pl.multiple_of(chunk_of(i) * per, per), per)

    def toward(way, hops):
        return (y + hops) % ny if way == 0 else (y + ny - hops) % ny

    def reach(way, hops, i):
        step, owner = (hops, y) if hops <= 2 else (hops - 2, toward(1 - way, 2))
        block = rows.at[chunk_rows(i), col(owner)]
        return remote(
            block, block, ag_ssem.at[way, hops - 1, i], ag_rsem.at[way, hops - 1, i],
            ep, toward(way, step) * nx + x,
        )

    def reached(way, hops, i):
        arrived(rows.at[chunk_rows(i), col(toward(1 - way, hops))], ag_rsem.at[way, hops - 1, i])

    def travels(way, hops, i):
        return hops < steps or (i < CHUNKS // 2) == (way == 0)

    def spread_near(i):
        if order[i] == 0:
            arrived(rows.at[pl.ds(0, per - cap), col(y)], z_recv.at[chunk_of(i)])
        else:
            arrived(rows.at[chunk_rows(i), col(y)], z_recv.at[chunk_of(i)])
        for hops in (2, 1):
            for way in (0, 1):
                launch(reach(way, hops, i))

    def spread_far(i):
        for way in (0, 1):
            reached(way, 2, i)
            for hops in (4, 3):
                if travels(way, hops, i):
                    launch(reach(way, hops, i))

    def partial(i):
        for hops in (1, 3, 4):
            for way in (0, 1):
                if travels(way, hops, i):
                    reached(way, hops, i)
        if i == 0:
            for d in range(1, nx):
                arrived(w_all.at[w_place((x + nx - d) % nx), :], w_rsem.at[d])
        block = rows[chunk_rows(i), :]
        for d in x_order + [0]:
            to = (x + d) % nx
            w_to = w_all[pl.ds(pl.multiple_of(to * LANES, LANES), LANES), :]
            part_send[i, :, col(to)] = dot(block, w_to, 1, 1).astype(BF16)
            if d == 0:
                break
            launch(
                remote(
                    part_send.at[i, :, col((x + d) % nx)], part_got.at[d, i],
                    px_ssem.at[d, i], px_rsem.at[d, i], ep, x_peer(d),
                )
            )
        if i == 0:
            for k in range(nx):
                top = slice(k * LANES, k * LANES + 2 * HID)
                rest = slice(k * LANES + 2 * HID, (k + 1) * LANES)
                w_left[top, :] = w_all[top, :]
                w_left[rest, :] = jnp.zeros((LANES - 2 * HID, ny * LANES), BF16)

    def activate(i):
        pre = part_send[i, :, col(x)].astype(F32)
        for d in range(1, nx):
            arrived(part_got.at[d, i], px_rsem.at[d, i])
            pre = pre + part_got[d, i].astype(F32)
        up = pltpu.roll(pre, LANES - HID, 1)
        d_hidden = pltpu.roll(pre, LANES - 2 * HID, 1)
        sig = jax.nn.sigmoid(pre)
        act = pre * sig * up
        d_gate = d_hidden * up * sig * (1.0 + pre * (1.0 - sig))
        d_up = d_hidden * pre * sig
        rw = jnp.sum(jnp.where(lane_c < HID, act * d_hidden, 0.0), axis=1, keepdims=True)
        tail = jnp.where(lane_c == 3 * HID, rw, 0.0)
        packed = jnp.where(lane_c < 3 * HID, pltpu.roll(act, 2 * HID, 1), tail)
        packed = jnp.where(lane_c < 2 * HID, pltpu.roll(d_up, HID, 1), packed)
        packed = jnp.where(lane_c < HID, d_gate, packed)
        mine = hidden.at[chunk_rows(i), col(x)]
        hidden[chunk_rows(i), col(x)] = packed.astype(BF16)
        for d in x_order:
            launch(remote(mine, mine, hx_ssem.at[d, i], hx_rsem.at[d, i], ep, x_peer(d)))

    def token_part(i):
        for d in range(1, nx):
            arrived(hidden.at[chunk_rows(i), col((x + nx - d) % nx)], hx_rsem.at[d, i])
        value = hidden[chunk_rows(i), :]
        whole = dot(value, w_left[...], 1, 0)
        for j in range(ny):
            tile = slice(j * LANES, (j + 1) * LANES)
            right = pltpu.roll(whole[pack:per, tile], FEAT, 1)
            piece[i, :, tile] = jnp.where(lane_p < FEAT, whole[0:pack, tile], right).astype(BF16)
        rw_row[i] = jnp.concatenate([dot(pick, value, 1, 1)[0:1, :]] * copies_wide, axis=1)
        for d in y_order:
            launch(
                remote(
                    piece.at[i, :, col((y + d) % ny)], piece_got.at[d, i],
                    ry_ssem.at[d, i], ry_rsem.at[d, i], ep, y_peer(d),
                )
            )
            launch(
                remote(rw_row.at[i], rw_got.at[d, i], rw_ssem.at[d, i], rw_rsem.at[d, i], ep, y_peer(d))
            )

    def send_back(to):
        remote(back.at[slot(to), :], back_got.at[slot(ep), :], b_ssem, b_rsem, to, tp).start()

    def summed(i):
        total = piece[i, :, col(y)].astype(F32)
        total_rw = rw_row[i]
        for d in y_order[::-1]:
            arrived(piece_got.at[d, i], ry_rsem.at[d, i])
            arrived(rw_got.at[d, i], rw_rsem.at[d, i])
            total = total + piece_got[d, i].astype(F32)
            total_rw = total_rw + rw_got[d, i]
        spread_rw = jnp.broadcast_to(total_rw, (LANES, LANES)).T[0:per, :]
        both_ = jnp.concatenate([total, pltpu.roll(total, FEAT, 1)], axis=0)
        back[chunk_rows(i), :] = jnp.where(lane_c < FEAT, both_, spread_rw).astype(BF16)
        base = chunk_of(i) * group
        if order[i] == 0:
            back_got[slot(ep), :] = back[slot(ep), :]
        for j in range(1 if order[i] == 0 else 0, group):
            send_back(base + (ep + j) % group)

    stages = [spread_near, spread_far, partial, activate, token_part, summed]
    after = [0, 4, 8, 13, 18, 26]
    apart = [2.5, 3, 3.5, 3.5, 3.5, 3.5]
    turns = sorted(
        (after[k] + apart[k] * i, k, i) for k in range(len(stages)) for i in range(CHUNKS)
    )
    for _, k, i in turns:
        if (k, i) == (len(stages) - 1, CHUNKS - 1):
            grads = dot(hidden[...], rows[...], 0, 0)
            g_lane = lax.broadcasted_iota(jnp.int32, (HID, ny * LANES), 1) % LANES
            for n in range(nx):
                at = n * LANES
                gate_down = jnp.where(
                    g_lane < FEAT, grads[at : at + HID, :], grads[at + 2 * HID : at + 3 * HID, :]
                )
                grad_send[n, 0:HID, :] = gate_down.astype(BF16)
                grad_send[n, HID : 2 * HID, :] = grads[at + HID : at + 2 * HID, :].astype(BF16)
            for d in range(1, nx):
                launch(
                    remote(
                        grad_send.at[(x + d) % nx], grad_got.at[x], g_ssem.at[d], g_rsem.at[d],
                        ep, x_peer(d),
                    )
                )
            grad_got[x] = grad_send[x]
        stages[k](i)

    for d in range(1, nx):
        arrived(grad_got.at[(x + nx - d) % nx], g_rsem.at[d])
    for t in range(0, nx * ny, 2):
        tile = slice(t // 2 * LANES, (t // 2 + 1) * LANES)
        src = slice(t // nx * LANES, (t // nx + 1) * LANES)
        a, b = t % nx, t % nx + 1
        top_a = grad_got[a, 0:HID, src].astype(F32)
        top_b = grad_got[b, 0:HID, src].astype(F32)
        up_a = grad_got[a, HID : 2 * HID, src].astype(F32)
        up_b = grad_got[b, HID : 2 * HID, src].astype(F32)
        out_gate[:, tile] = jnp.where(w_lane < FEAT, top_a, pltpu.roll(top_b, FEAT, 1))
        out_up[:, tile] = jnp.where(w_lane < FEAT, up_a, pltpu.roll(up_b, FEAT, 1))
        out_down[:, tile] = jnp.where(w_lane < FEAT, pltpu.roll(top_a, FEAT, 1), top_b)

    stores = [
        pltpu.make_async_copy(out_tok, out_hbm0, out_sem.at[0]),
        pltpu.make_async_copy(out_rw, out_hbm1, out_sem.at[1]),
        pltpu.make_async_copy(out_gate, out_hbm2, out_sem.at[2]),
        pltpu.make_async_copy(out_up, out_hbm3, out_sem.at[3]),
        pltpu.make_async_copy(out_down, out_hbm4, out_sem.at[4]),
    ]
    for copy in stores[2:]:
        copy.start()
    others = pl.ds(0, (nep - 1) * cap)
    arrived(back_got.at[others, :], b_rsem)
    got = back_got[...]
    by_first = dot(got, onehot0[...], 0, 0)
    by_second = dot(got, onehot1[...], 0, 0)
    out_tok[...] = (by_first[0:FEAT, :] + by_second[0:FEAT, :]).astype(BF16)
    out_rw[0:1, :] = by_first[FEAT : FEAT + 1, :] / weights[0:1, :]
    out_rw[1:2, :] = by_second[FEAT : FEAT + 1, :] / weights[1:2, :]

    for copy in stores[:2]:
        copy.start()
    arrived(send.at[others, :], z_send)
    arrived(back.at[others, :], b_ssem)
    for copy in w_copies + copies:
        copy.wait_send()
    for copy in stores:
        copy.wait()


def store(*refs):
    given, kept, held, sems = refs[0:5], refs[5:10], refs[10:15], refs[15]
    loads = [pltpu.make_async_copy(given[i], held[i], sems.at[0, i]) for i in range(5)]
    stores = [pltpu.make_async_copy(held[i], kept[i], sems.at[1, i]) for i in range(5)]
    for copy in loads:
        copy.start()
    for load, copy in zip(loads, stores):
        load.wait()
        copy.start()
    for copy in stores:
        copy.wait()


def on_device(nz, ny, nx, tokens, cotangent, routes, route_weight, w_gate, w_up, w_down):
    tok_dev, model = tokens.shape
    hid = w_down.shape[1]
    nep = 2 * nz
    cap = 2 * tok_dev * routes.shape[1] // nep
    count = nep * cap
    per = count // CHUNKS
    wide_x, wide_y = nx * LANES, ny * LANES
    steps = ny // 2
    hbm = pl.BlockSpec(memory_space=pltpu.HBM)
    dma = pltpu.SemaphoreType.DMA
    outs = pl.pallas_call(
        functools.partial(kernel, nz, ny, nx, cap),
        out_shape=(
            jax.ShapeDtypeStruct((FEAT, tok_dev), BF16),
            jax.ShapeDtypeStruct((2, tok_dev), F32),
            jax.ShapeDtypeStruct((hid, model), F32),
            jax.ShapeDtypeStruct((hid, model), F32),
            jax.ShapeDtypeStruct((hid, model), F32),
        ),
        in_specs=[hbm] * 7,
        out_specs=[hbm] * 5,
        scratch_shapes=[
            pltpu.VMEM((tok_dev, LANES), BF16),
            pltpu.VMEM((tok_dev, LANES), BF16),
            pltpu.VMEM((hid, model), BF16),
            pltpu.VMEM((hid, model), BF16),
            pltpu.VMEM((hid, model), BF16),
            pltpu.VMEM((2, tok_dev), jnp.int32),
            pltpu.VMEM((2, tok_dev), F32),
            pltpu.VMEM((count, tok_dev), BF16),
            pltpu.VMEM((count, tok_dev), BF16),
            pltpu.VMEM((count, LANES), BF16),
            pltpu.VMEM((count, wide_y), BF16),
            pltpu.VMEM((nx, 3 * HID, wide_y), BF16),
            pltpu.VMEM((wide_x, wide_y), BF16),
            pltpu.VMEM((wide_x, wide_y), BF16),
            pltpu.VMEM((CHUNKS, per, wide_x), BF16),
            pltpu.VMEM((nx, CHUNKS, per, LANES), BF16),
            pltpu.VMEM((count, wide_x), BF16),
            pltpu.VMEM((CHUNKS, per // 2, wide_y), BF16),
            pltpu.VMEM((ny, CHUNKS, per // 2, LANES), BF16),
            pltpu.VMEM((CHUNKS, 1, LANES), F32),
            pltpu.VMEM((ny, CHUNKS, 1, LANES), F32),
            pltpu.VMEM((count, LANES), BF16),
            pltpu.VMEM((count, LANES), BF16),
            pltpu.VMEM((nx, 2 * HID, wide_y), BF16),
            pltpu.VMEM((nx, 2 * HID, wide_y), BF16),
            dma((7,)),
            dma,
            dma((CHUNKS,)),
            dma((nx,)),
            dma((nx,)),
            dma((2, steps, CHUNKS)),
            dma((2, steps, CHUNKS)),
            dma((nx, CHUNKS)),
            dma((nx, CHUNKS)),
            dma((nx, CHUNKS)),
            dma((nx, CHUNKS)),
            dma((ny, CHUNKS)),
            dma((ny, CHUNKS)),
            dma((ny, CHUNKS)),
            dma((ny, CHUNKS)),
            dma,
            dma,
            dma((nx,)),
            dma((nx,)),
            pltpu.VMEM((FEAT, tok_dev), BF16),
            pltpu.VMEM((2, tok_dev), F32),
            pltpu.VMEM((hid, model), F32),
            pltpu.VMEM((hid, model), F32),
            pltpu.VMEM((hid, model), F32),
            dma((5,)),
        ],
        compiler_params=pltpu.CompilerParams(
            collective_id=0, has_side_effects=True, vmem_limit_bytes=62 * 1024 * 1024
        ),
        name="experts_backward",
    )(
        tokens,
        cotangent,
        routes.T,
        route_weight.T,
        w_gate[0].T,
        w_up[0].T,
        w_down[0],
    )
    g_tok, g_rw, g_gate, g_up, g_down = pl.pallas_call(
        store,
        out_shape=tuple(jax.ShapeDtypeStruct(o.shape, o.dtype) for o in outs),
        in_specs=[hbm] * 5,
        out_specs=[hbm] * 5,
        scratch_shapes=[pltpu.VMEM(o.shape, o.dtype) for o in outs] + [dma((2, 5))],
        compiler_params=pltpu.CompilerParams(vmem_limit_bytes=62 * 1024 * 1024),
        name="store",
    )(*outs)
    return g_tok.T, g_rw.T, g_gate.T[None], g_up.T[None], g_down[None]


def solution(mesh):
    nz = mesh.shape["ep"] // 2
    nx = 4 if mesh.shape["tp"] >= 16 else 2
    ny = mesh.shape["tp"] // nx
    return jax.shard_map(
        functools.partial(on_device, nz, ny, nx),
        mesh=mesh,
        in_specs=(
            P("ep", None),
            P("ep", None),
            P("ep", None),
            P("ep", None),
            P("ep", None, "tp"),
            P("ep", None, "tp"),
            P("ep", "tp", None),
        ),
        out_specs=(
            P("ep", "tp"),
            P("ep", None),
            P("ep", None, "tp"),
            P("ep", None, "tp"),
            P("ep", "tp", None),
        ),
        check_vma=False,
    )
```
